32 devices in a mesh: dp: 4 (over y, x), kv: 4 (over z), tp: 2 (over core).
Axes of the slice: x: 2, y: 2, z: 4, core: 2. Of those that a mesh axis runs over, the one named last changes fastest.
Arguments:
- tokens: bfloat16 [32, 4096], P('dp', ('kv', 'tp')), may hold values from -7 to 7
- mix_gain: float32 [4096], replicated, may hold values from 0.1 to 1.9
- query_weight: bfloat16 [16, 128, 4096], P('tp', 'kv'), may hold values from -0.09375 to 0.09375
- forget_weight: bfloat16 [16, 128, 4096], P('tp', 'kv'), may hold values from -0.09375 to 0.09375
- value_weight: bfloat16 [16, 128, 4096], P('tp', 'kv'), may hold values from -0.09375 to 0.09375
- gate_weight: bfloat16 [16, 128, 4096], P('tp', 'kv'), may hold values from -0.09375 to 0.09375
- lower_bound: float32 [16, 128], P('tp'), may hold values from 0.02 to 0.9
- recurrent_state: float32 [32, 16, 128, 128], P(('dp', 'kv'), 'tp'), may hold values from -3 to 3
- head_gain: float32 [16, 128], P('tp'), may hold values from 0.1 to 1.9
- out_weight: bfloat16 [16, 128, 4096], P(None, None, ('kv', 'tp')), may hold values from -0.125 to 0.125
- mlp_gain: float32 [4096], replicated, may hold values from 0.1 to 1.9
- up_weight: bfloat16 [4096, 16384], P(None, ('kv', 'tp')), may hold values from -0.09375 to 0.09375
- down_weight: bfloat16 [16384, 4096], P(('kv', 'tp')), may hold values from -0.0625 to 0.0625
Outputs:
- layer_output: bfloat16 [32, 4096], P('dp', ('kv', 'tp'))
- next_state: float32 [32, 16, 128, 128], P(('dp', 'kv'), 'tp')
The draws below stay inside these ranges and needn't reach their ends.
All inputs are finite; a program needn't handle non-finite values.
Results may differ from the reference program's by a relative error of at most 0.0072.
Values may be sent and summed in bfloat16 or wider, within the bound.
No kernel may reach another device: no remote copies, remote signals or barrier semaphores. Data moves between devices by JAX's collectives and lax.ppermute only.
A program may use at most 128 MiB of HBM per device.

```python
import math
import jax
import jax.numpy as jnp
from jax import lax

D = 4096
HEADS = 16
KEY_DIM = 128
VALUE_DIM = 128
FF = 16384
BATCH = 32


def draw_tokens(key, part):
    noise_key = jax.random.fold_in(jax.random.fold_in(key, 17), 0)
    column = jnp.arange(D, dtype=jnp.float32) / (D - 1)
    values = jnp.clip(jax.random.normal(noise_key, (BATCH, D), jnp.float32), -4.0, 4.0)
    spread = math.log(3.0)
    scaled = values * jnp.exp(spread * (column - 0.5))
    return scaled.astype(jnp.bfloat16)


def raised(entries, own_key, source, target, shards_of, factor):
    def block_of(axis_at):
        return (jnp.arange(entries.shape[axis_at]) // (entries.shape[axis_at] // shards_of)).reshape((-1,) + (1,) * (entries.ndim - 1 - axis_at))

    first = jax.random.permutation(own_key, shards_of)[block_of(target)]
    other_side = (block_of(target) + shards_of // 2) % shards_of
    return jnp.where((block_of(source) == first) | (block_of(source) == other_side), factor * entries, entries)


def level_of(own_key, extent, pieces, low, largest):
    loudness = 1.0
    for dim, shards_of in pieces:
        draws = jax.random.uniform(jax.random.fold_in(jax.random.fold_in(own_key, 6), dim), (shards_of,), jnp.float32, low / len(pieces), largest / len(pieces))
        loudness = loudness * jnp.repeat(jnp.exp(draws), extent[dim] // shards_of).reshape((-1,) + (1,) * (len(extent) - 1 - dim))
    return loudness


def centred(own_key, dims, deviation, limit, cuts=(), kind=jnp.bfloat16):
    level = level_of(own_key, dims, cuts, -0.22, 0.18) if cuts else 1.0
    drawn = jax.random.normal(own_key, dims, jnp.float32) * deviation * level
    return jnp.minimum(jnp.maximum(drawn, -limit), limit).astype(kind)


def gaussian_with(stream_key, dims, deviation, bound, pieces, heavy, held_as=jnp.bfloat16):
    drawn = deviation * jax.random.normal(stream_key, dims, jnp.float32)
    if pieces:
        drawn = drawn * level_of(stream_key, dims, pieces, -0.22, 0.18)
    return jnp.clip(raised(drawn, jax.random.fold_in(stream_key, 3), *heavy), -bound, bound).astype(held_as)


def setup_inputs(seed: int = 0) -> dict:
    key_of = jax.random.split(jax.random.key(seed), 14)
    return {
        "tokens": draw_tokens(jax.random.fold_in(key_of[13], 71), 0),
        "mix_gain": jnp.clip(1.0 + 0.18 * jax.random.normal(key_of[1], (D,), jnp.float32), 0.1, 1.9),
        "query_weight": centred(key_of[2], (HEADS, KEY_DIM, D), D ** -0.5, 0.09375, ((0, 2), (1, 4))),
        "forget_weight": centred(key_of[3], (HEADS, KEY_DIM, D), D ** -0.5, 0.09375, ((0, 2), (1, 4))),
        "value_weight": centred(key_of[4], (HEADS, VALUE_DIM, D), D ** -0.5, 0.09375, ((0, 2), (1, 4))),
        "gate_weight": centred(key_of[5], (HEADS, VALUE_DIM, D), D ** -0.5, 0.09375, ((0, 2), (1, 4))),
        "lower_bound": jnp.clip(jnp.exp(math.log(0.9) - 3.8066625 * jax.random.uniform(key_of[6], (HEADS, KEY_DIM), jnp.float32) ** level_of(key_of[6], (HEADS, KEY_DIM), ((0, 2),), -0.2, 0.2)), 0.02, 0.9),
        "recurrent_state": centred(key_of[7], (BATCH, HEADS, KEY_DIM, VALUE_DIM), 0.5, 3.0, ((0, 16), (1, 2)), jnp.float32),
        "head_gain": jnp.clip(1.0 + 0.18 * jax.random.normal(key_of[8], (HEADS, VALUE_DIM), jnp.float32), 0.1, 1.9),
        "out_weight": centred(key_of[9], (HEADS, VALUE_DIM, D), (HEADS * VALUE_DIM) ** -0.5, 0.125, ((2, 8),)),
        "mlp_gain": jnp.clip(1.0 + 0.18 * jax.random.normal(key_of[10], (D,), jnp.float32), 0.1, 1.9),
        "up_weight": centred(key_of[11], (D, FF), D ** -0.5, 0.09375, ((1, 8),)),
        "down_weight": gaussian_with(key_of[12], (FF, D), FF ** -0.5, 0.0625, ((0, 8),), (0, 1, 8, 2.0)),
    }


epsilon = 1e-06

def rms_rows(matrix, gain_vector):
    as_float = matrix.astype(jnp.float32)
    inv_root = lax.rsqrt(lax.optimization_barrier(jnp.mean(as_float * as_float, axis=1, keepdims=True)) + epsilon)
    return (as_float * inv_root * gain_vector).astype(jnp.bfloat16)

def project_rows(normed, weight):
    flat_weight = weight.reshape(-1, weight.shape[2])
    product = lax.dot_general(normed, flat_weight, (((1,), (1,)), ((), ())), preferred_element_type=jnp.float32).astype(jnp.bfloat16)
    return product.reshape(normed.shape[0], weight.shape[0], weight.shape[1])

def reference(tokens, mix_gain, query_weight, forget_weight, value_weight, gate_weight, lower_bound, recurrent_state, head_gain, out_weight, mlp_gain, up_weight, down_weight):
    normed = rms_rows(tokens, mix_gain)
    pre_query, pre_forget, value_rows, pre_gate = lax.optimization_barrier((project_rows(normed, query_weight), project_rows(normed, forget_weight), project_rows(normed, value_weight), project_rows(normed, gate_weight)))
    log_forget = jnp.logaddexp(jnp.log(lower_bound), jnp.log1p(-lower_bound) + jax.nn.log_sigmoid(pre_forget.astype(jnp.float32)))
    key_rows = -jnp.expm1(log_forget)
    next_state = jnp.exp(log_forget)[:, :, :, None] * recurrent_state + key_rows[:, :, :, None] * value_rows.astype(jnp.float32)[:, :, None, :]
    query_act = jax.nn.silu(pre_query.astype(jnp.float32))
    readout = jnp.einsum('bhk,bhkv->bhv', query_act, next_state, precision=lax.Precision.HIGHEST)
    inv_head = lax.rsqrt(lax.optimization_barrier(jnp.mean(readout * readout, axis=2, keepdims=True)) + epsilon)
    mixed_heads = (readout * inv_head * head_gain * jax.nn.silu(pre_gate.astype(jnp.float32))).astype(jnp.bfloat16)
    projected = jnp.dot(mixed_heads.reshape(mixed_heads.shape[0], -1), out_weight.reshape(-1, out_weight.shape[2]), preferred_element_type=jnp.float32)
    residual = lax.optimization_barrier((tokens.astype(jnp.float32) + projected).astype(jnp.bfloat16))
    normed_mlp = rms_rows(residual, mlp_gain)
    hidden = jnp.square(jax.nn.relu(jnp.dot(normed_mlp, up_weight, preferred_element_type=jnp.float32))).astype(jnp.bfloat16)
    layer_output = (residual.astype(jnp.float32) + jnp.dot(hidden, down_weight, preferred_element_type=jnp.float32)).astype(jnp.bfloat16)
    return (layer_output, next_state)
```

```python
import jax
import jax.numpy as jnp
from jax import lax
from jax.sharding import PartitionSpec as P

epsilon = 1e-06
group = ("kv", "tp")


def gather_blocks(block, members):
    copies = lax.optimization_barrier(jnp.broadcast_to(block[None], (members,) + block.shape))
    return lax.all_to_all(copies, group, split_axis=0, concat_axis=0, tiled=True)


def whole_rows(row_block, members):
    pieces = gather_blocks(row_block, members)
    return jnp.swapaxes(pieces, 0, 1).reshape(row_block.shape[0], -1)


def normed_rows(rows, gain_vector):
    rows = rows.astype(jnp.float32)
    inv_root = lax.rsqrt(jnp.mean(rows * rows, axis=1, keepdims=True) + epsilon)
    return (rows * inv_root * gain_vector).astype(jnp.bfloat16)


def local(
    kv,
    tp,
    tokens,
    mix_gain,
    query_weight,
    forget_weight,
    value_weight,
    gate_weight,
    lower_bound,
    recurrent_state,
    head_gain,
    out_weight,
    mlp_gain,
    up_weight,
    down_weight,
):
    members = kv * tp
    normed = normed_rows(whole_rows(tokens, members), mix_gain)
    local_heads, local_chan, width = query_weight.shape
    rows = normed.shape[0]
    own_rows = rows // kv
    products = [
        lax.dot_general(
            normed,
            weight.reshape(-1, width),
            (((1,), (1,)), ((), ())),
            preferred_element_type=jnp.float32,
        ).astype(jnp.bfloat16)
        for weight in (query_weight, forget_weight, value_weight, gate_weight)
    ]
    product = jnp.stack(products, axis=1).reshape(kv, own_rows * 4 * local_heads, local_chan)
    exchanged = lax.all_to_all(product, "kv", split_axis=0, concat_axis=0, tiled=True)
    channels = jnp.moveaxis(exchanged.reshape(kv, own_rows, 4, local_heads, local_chan), 0, 3)
    channels = channels.reshape(own_rows, 4, local_heads, kv * local_chan).astype(jnp.float32)
    pre_query, pre_forget, value_rows, pre_gate = (channels[:, i] for i in range(4))
    log_forget = jnp.logaddexp(
        jnp.log(lower_bound),
        jnp.log1p(-lower_bound) + jax.nn.log_sigmoid(pre_forget),
    )
    key_rows = -jnp.expm1(log_forget)
    next_state = (
        jnp.exp(log_forget)[:, :, :, None] * recurrent_state
        + key_rows[:, :, :, None] * value_rows[:, :, None, :]
    )
    query_act = jax.nn.silu(pre_query)
    readout = jnp.einsum("bhk,bhkv->bhv", query_act, next_state, precision=lax.Precision.HIGHEST)
    inv_head = lax.rsqrt(jnp.mean(readout * readout, axis=2, keepdims=True) + epsilon)
    mixed_heads = (readout * inv_head * head_gain * jax.nn.silu(pre_gate)).astype(jnp.bfloat16)
    mixed = gather_blocks(mixed_heads.reshape(own_rows, -1), members)
    mixed = jnp.swapaxes(mixed.reshape(kv, tp, own_rows, -1), 1, 2).reshape(rows, -1)
    out_matrix = out_weight.reshape(-1, out_weight.shape[2])
    projected = jnp.dot(mixed, out_matrix, preferred_element_type=jnp.float32)
    residual = lax.optimization_barrier(
        (tokens.astype(jnp.float32) + projected).astype(jnp.bfloat16)
    )
    normed_mlp = normed_rows(whole_rows(residual, members), mlp_gain)
    hidden = jnp.square(
        jax.nn.relu(jnp.dot(normed_mlp, up_weight, preferred_element_type=jnp.float32))
    ).astype(jnp.bfloat16)
    partial = jnp.dot(hidden, down_weight, preferred_element_type=jnp.float32)
    partial = jnp.swapaxes(partial.reshape(rows, members, -1), 0, 1)
    summed = lax.all_to_all(partial, group, split_axis=0, concat_axis=0, tiled=True).sum(axis=0)
    layer_output = (residual.astype(jnp.float32) + summed).astype(jnp.bfloat16)
    return (layer_output, next_state)


def solution(mesh):
    placed = (
        P("dp", ("kv", "tp")),
        P(),
        P("tp", "kv", None),
        P("tp", "kv", None),
        P("tp", "kv", None),
        P("tp", "kv", None),
        P("tp", None),
        P(("dp", "kv"), "tp", None, None),
        P("tp", None),
        P(None, None, ("kv", "tp")),
        P(),
        P(None, ("kv", "tp")),
        P(("kv", "tp"), None),
    )

    def body(*arrays):
        return local(mesh.shape["kv"], mesh.shape["tp"], *arrays)

    return jax.shard_map(
        body,
        mesh=mesh,
        in_specs=placed,
        out_specs=(P("dp", ("kv", "tp")), P(("dp", "kv"), "tp", None, None)),
        check_vma=False,
    )
```

```python
import functools

import jax
import jax.numpy as jnp
from jax import lax
from jax.experimental import pallas as pl
from jax.experimental.pallas import tpu as pltpu
from jax.sharding import PartitionSpec as P

epsilon = 1e-06
group = ("kv", "tp")


def gather_blocks(block, members):
    copies = lax.optimization_barrier(jnp.broadcast_to(block[None], (members,) + block.shape))
    return lax.all_to_all(copies, group, split_axis=0, concat_axis=0, tiled=True)


def whole_rows(row_block, members):
    pieces = gather_blocks(row_block, members)
    return jnp.swapaxes(pieces, 0, 1).reshape(row_block.shape[0], -1)


def normed_rows(rows, gain_vector):
    rows = rows.astype(jnp.float32)
    inv_root = lax.rsqrt(jnp.mean(rows * rows, axis=1, keepdims=True) + epsilon)
    return (rows * inv_root * gain_vector).astype(jnp.bfloat16)


def local(
    kv,
    tp,
    tokens,
    mix_gain,
    query_weight,
    forget_weight,
    value_weight,
    gate_weight,
    lower_bound,
    recurrent_state,
    head_gain,
    out_weight,
    mlp_gain,
    up_weight,
    down_weight,
):
    members = kv * tp
    normed = normed_rows(whole_rows(tokens, members), mix_gain)
    local_heads, local_chan, width = query_weight.shape
    rows = normed.shape[0]
    own_rows = rows // kv
    products = [
        lax.dot_general(
            normed,
            weight.reshape(-1, width),
            (((1,), (1,)), ((), ())),
            preferred_element_type=jnp.float32,
        ).astype(jnp.bfloat16)
        for weight in (query_weight, forget_weight, value_weight, gate_weight)
    ]
    product = jnp.stack(products, axis=1).reshape(kv, own_rows * 4 * local_heads, local_chan)
    exchanged = lax.all_to_all(product, "kv", split_axis=0, concat_axis=0, tiled=True)
    channels = jnp.moveaxis(exchanged.reshape(kv, own_rows, 4, local_heads, local_chan), 0, 3)
    channels = channels.reshape(own_rows, 4, local_heads, kv * local_chan).astype(jnp.float32)
    pre_query, pre_forget, value_rows, pre_gate = (channels[:, i] for i in range(4))
    log_forget = jnp.logaddexp(
        jnp.log(lower_bound),
        jnp.log1p(-lower_bound) + jax.nn.log_sigmoid(pre_forget),
    )
    key_rows = -jnp.expm1(log_forget)
    next_state = (
        jnp.exp(log_forget)[:, :, :, None] * recurrent_state
        + key_rows[:, :, :, None] * value_rows[:, :, None, :]
    )
    query_act = jax.nn.silu(pre_query)
    readout = jnp.einsum("bhk,bhkv->bhv", query_act, next_state, precision=lax.Precision.HIGHEST)
    inv_head = lax.rsqrt(jnp.mean(readout * readout, axis=2, keepdims=True) + epsilon)
    mixed_heads = (readout * inv_head * head_gain * jax.nn.silu(pre_gate)).astype(jnp.bfloat16)
    mixed = gather_blocks(mixed_heads.reshape(own_rows, -1), members)
    mixed = jnp.swapaxes(mixed.reshape(kv, tp, own_rows, -1), 1, 2).reshape(rows, -1)
    out_matrix = out_weight.reshape(-1, out_weight.shape[2])
    projected = jnp.dot(mixed, out_matrix, preferred_element_type=jnp.float32)
    residual = lax.optimization_barrier(
        (tokens.astype(jnp.float32) + projected).astype(jnp.bfloat16)
    )
    normed_mlp = normed_rows(whole_rows(residual, members), mlp_gain)
    hidden = jnp.square(
        jax.nn.relu(jnp.dot(normed_mlp, up_weight, preferred_element_type=jnp.float32))
    ).astype(jnp.bfloat16)
    partial = jnp.dot(hidden, down_weight, preferred_element_type=jnp.float32)
    partial = jnp.swapaxes(partial.reshape(rows, members, -1), 0, 1)
    summed = lax.all_to_all(partial, group, split_axis=0, concat_axis=0, tiled=True).sum(axis=0)
    layer_output = (residual.astype(jnp.float32) + summed).astype(jnp.bfloat16)
    return (layer_output, next_state)


whole = pl.BlockSpec(memory_space=pltpu.VMEM)


def call(body, outs, arrays, flops, moved, limit):
    return pl.pallas_call(
        body,
        out_shape=outs,
        in_specs=[whole] * len(arrays),
        out_specs=jax.tree.map(lambda _: whole, outs),
        compiler_params=pltpu.CompilerParams(vmem_limit_bytes=limit),
        cost_estimate=pl.CostEstimate(flops=flops, bytes_accessed=moved, transcendentals=0),
    )(*arrays)


def spread_kernel(block_ref, copies_ref):
    for dest in range(copies_ref.shape[0]):
        copies_ref[dest] = block_ref[...]


def normed_pieces(pieces_ref, gain_ref):
    rows = jnp.concatenate([pieces_ref[i] for i in range(pieces_ref.shape[0])], axis=1)
    rows = rows.astype(jnp.float32)
    inv_root = lax.rsqrt(jnp.mean(rows * rows, axis=1, keepdims=True) + epsilon)
    return (rows * inv_root * gain_ref[...]).astype(jnp.bfloat16)


def project_kernel(pieces_ref, gain_ref, query_ref, forget_ref, value_ref, gate_ref, sent_ref):
    normed = normed_pieces(pieces_ref, gain_ref)
    rows = normed.shape[0]
    heads, chan, _ = query_ref.shape
    lanes = 4 * chan
    for head in range(0, heads, 2):
        weight = jnp.concatenate(
            [
                ref[one]
                for one in (head, head + 1)
                for ref in (query_ref, forget_ref, value_ref, gate_ref)
            ],
            axis=0,
        )
        product = lax.dot_general(
            normed, weight, (((1,), (1,)), ((), ())), preferred_element_type=jnp.float32
        )
        product = product.astype(jnp.bfloat16).astype(jnp.float32)
        sent_ref[pl.ds(head, rows, stride=heads), :] = product[:, :lanes]
        sent_ref[pl.ds(head + 1, rows, stride=heads), :] = product[:, lanes:]


def sigmoid(x):
    return 1.0 / (1.0 + jnp.exp(-x))


def state_kernel(got_ref, bound_ref, state_ref, gain_ref, next_ref, copies_ref):
    sources, pairs, _ = got_ref.shape
    own_rows, heads, keys, values = state_ref.shape
    chan = keys // sources

    def channels(kind):
        return jnp.concatenate(
            [got_ref[i][:, kind * chan : (kind + 1) * chan] for i in range(sources)], axis=1
        )

    pre_query, pre_forget, value_rows, pre_gate = (channels(kind) for kind in range(4))
    bound = jnp.concatenate([bound_ref[...]] * own_rows, axis=0)
    gain = jnp.concatenate([gain_ref[...]] * own_rows, axis=0)
    forget = jnp.transpose(bound + (1.0 - bound) * sigmoid(pre_forget))
    key_cols = jnp.transpose((1.0 - bound) * sigmoid(-pre_forget))
    query = jnp.transpose(pre_query * sigmoid(pre_query))
    readouts = []
    for row in range(own_rows):
        for head in range(heads):
            pair = row * heads + head
            one = slice(pair, pair + 1)
            state = forget[:, one] * state_ref[row, head] + key_cols[:, one] * value_rows[one]
            next_ref[row, head] = state
            readouts.append(jnp.sum(query[:, one] * state, axis=0, keepdims=True))
    readout = jnp.concatenate(readouts, axis=0)
    inv_head = lax.rsqrt(jnp.mean(readout * readout, axis=1, keepdims=True) + epsilon)
    mixed = readout * inv_head * gain * (pre_gate * sigmoid(pre_gate))
    mixed = mixed.astype(jnp.bfloat16).astype(jnp.float32)
    for dest in range(copies_ref.shape[0]):
        copies_ref[dest] = mixed


def out_kernel(kv, tp, heads, tokens_ref, mixed_ref, weight_ref, copies_ref, residual_ref):
    pairs, rows = mixed_ref.shape[0] // (kv * tp), tokens_ref.shape[0]
    own_rows = pairs // heads
    blocks = []
    for part in range(tp):
        for head in range(heads):
            blocks.append(
                jnp.concatenate(
                    [
                        mixed_ref[pl.ds(part * pairs + row * heads + head, kv, stride=tp * pairs), :]
                        for row in range(own_rows)
                    ],
                    axis=0,
                )
            )
    mixed = jnp.concatenate(blocks, axis=1).astype(jnp.bfloat16)
    width = weight_ref.shape[2]
    weight = weight_ref[...].reshape(-1, width)
    projected = jnp.dot(mixed, weight, preferred_element_type=jnp.float32)
    ordered = [
        projected[row * kv + i : row * kv + i + 1] for i in range(kv) for row in range(own_rows)
    ]
    projected = jnp.concatenate(ordered, axis=0)
    residual = (tokens_ref[...].astype(jnp.float32) + projected).astype(jnp.bfloat16)
    residual_ref[...] = residual
    for dest in range(copies_ref.shape[0]):
        copies_ref[dest] = residual


def mixer_kernel(pieces_ref, gain_ref, up_ref, down_ref, partial_ref):
    members, _, width = partial_ref.shape
    normed = normed_pieces(pieces_ref, gain_ref)
    hidden = jnp.dot(normed, up_ref[...], preferred_element_type=jnp.float32)
    hidden = jnp.square(jnp.maximum(hidden, 0.0)).astype(jnp.bfloat16)
    for dest in range(members):
        partial_ref[dest] = jnp.dot(
            hidden,
            down_ref[:, dest * width : (dest + 1) * width],
            preferred_element_type=jnp.float32,
        )


def last_kernel(residual_ref, partial_ref, output_ref):
    total = partial_ref[0]
    for source in range(1, partial_ref.shape[0]):
        total = total + partial_ref[source]
    output_ref[...] = (residual_ref[...].astype(jnp.float32) + total).astype(jnp.bfloat16)


MIB = 1 << 20


def tiled_local(
    kv,
    tp,
    tokens,
    mix_gain,
    query_weight,
    forget_weight,
    value_weight,
    gate_weight,
    lower_bound,
    recurrent_state,
    head_gain,
    out_weight,
    mlp_gain,
    up_weight,
    down_weight,
):
    members = kv * tp
    rows, width = tokens.shape
    heads, chan, model = query_weight.shape
    own_rows, _, keys, values = recurrent_state.shape
    pairs = own_rows * heads
    shape = jax.ShapeDtypeStruct
    exchange = functools.partial(lax.all_to_all, split_axis=0, concat_axis=0, tiled=True)

    copies = call(
        spread_kernel, shape((members, rows, width), jnp.bfloat16), (tokens,), COST[0], 0, MIB
    )
    pieces = exchange(copies, group)
    sent = call(
        project_kernel,
        shape((rows * heads, 4 * chan), jnp.float32),
        (
            pieces,
            mix_gain.reshape(1, -1),
            query_weight,
            forget_weight,
            value_weight,
            gate_weight,
        ),
        COST[1],
        0,
        4 * MIB,
    )
    got = exchange(sent.reshape(kv, pairs, 4 * chan), "kv")
    next_state, copies = call(
        state_kernel,
        (
            shape(recurrent_state.shape, jnp.float32),
            shape((members, pairs, values), jnp.float32),
        ),
        (got, lower_bound, recurrent_state, head_gain),
        COST[2],
        0,
        4 * MIB,
    )
    mixed = exchange(copies, group)
    copies, residual = call(
        functools.partial(out_kernel, kv, tp, heads),
        (shape((members, rows, width), jnp.bfloat16), shape((rows, width), jnp.bfloat16)),
        (tokens, mixed.reshape(members * pairs, values), out_weight),
        COST[3],
        0,
        4 * MIB,
    )
    pieces = exchange(copies, group)
    partial = call(
        mixer_kernel,
        shape((members, rows, width), jnp.float32),
        (pieces, mlp_gain.reshape(1, -1), up_weight, down_weight),
        COST[4],
        0,
        4 * MIB,
    )
    partial = exchange(partial, group)
    layer_output = call(
        last_kernel, shape((rows, width), jnp.bfloat16), (residual, partial), COST[5], 0, MIB
    )
    return (layer_output, next_state)


COST = (10**11, 10**11, 10**11, 10**6, 10**6, 10**6)


def tiles(tokens, query_weight):
    rows, width = tokens.shape
    return rows % 8 == 0 and width % 128 == 0 and query_weight.shape[1] % 32 == 0


def solution(mesh):
    placed = (
        P("dp", ("kv", "tp")),
        P(),
        P("tp", "kv", None),
        P("tp", "kv", None),
        P("tp", "kv", None),
        P("tp", "kv", None),
        P("tp", None),
        P(("dp", "kv"), "tp", None, None),
        P("tp", None),
        P(None, None, ("kv", "tp")),
        P(),
        P(None, ("kv", "tp")),
        P(("kv", "tp"), None),
    )

    def body(*arrays):
        run = tiled_local if tiles(arrays[0], arrays[2]) else local
        return run(mesh.shape["kv"], mesh.shape["tp"], *arrays)

    return jax.shard_map(
        body,
        mesh=mesh,
        in_specs=placed,
        out_specs=(P("dp", ("kv", "tp")), P(("dp", "kv"), "tp", None, None)),
        check_vma=False,
    )
```

```python
import functools

import jax
import jax.numpy as jnp
from jax import lax
from jax.experimental import pallas as pl
from jax.experimental.pallas import tpu as pltpu
from jax.sharding import PartitionSpec as P


epsilon = 1e-06
group = ("kv", "tp")


def gather_blocks(block, members):
    copies = lax.optimization_barrier(jnp.broadcast_to(block[None], (members,) + block.shape))
    return lax.all_to_all(copies, group, split_axis=0, concat_axis=0, tiled=True)


def whole_rows(row_block, members):
    pieces = gather_blocks(row_block, members)
    return jnp.swapaxes(pieces, 0, 1).reshape(row_block.shape[0], -1)


def normed_rows(rows, gain_vector):
    rows = rows.astype(jnp.float32)
    inv_root = lax.rsqrt(jnp.mean(rows * rows, axis=1, keepdims=True) + epsilon)
    return (rows * inv_root * gain_vector).astype(jnp.bfloat16)


def local(
    kv,
    tp,
    tokens,
    mix_gain,
    query_weight,
    forget_weight,
    value_weight,
    gate_weight,
    lower_bound,
    recurrent_state,
    head_gain,
    out_weight,
    mlp_gain,
    up_weight,
    down_weight,
):
    members = kv * tp
    normed = normed_rows(whole_rows(tokens, members), mix_gain)
    local_heads, local_chan, width = query_weight.shape
    rows = normed.shape[0]
    own_rows = rows // kv
    products = [
        lax.dot_general(
            normed,
            weight.reshape(-1, width),
            (((1,), (1,)), ((), ())),
            preferred_element_type=jnp.float32,
        ).astype(jnp.bfloat16)
        for weight in (query_weight, forget_weight, value_weight, gate_weight)
    ]
    product = jnp.stack(products, axis=1).reshape(kv, own_rows * 4 * local_heads, local_chan)
    exchanged = lax.all_to_all(product, "kv", split_axis=0, concat_axis=0, tiled=True)
    channels = jnp.moveaxis(exchanged.reshape(kv, own_rows, 4, local_heads, local_chan), 0, 3)
    channels = channels.reshape(own_rows, 4, local_heads, kv * local_chan).astype(jnp.float32)
    pre_query, pre_forget, value_rows, pre_gate = (channels[:, i] for i in range(4))
    log_forget = jnp.logaddexp(
        jnp.log(lower_bound),
        jnp.log1p(-lower_bound) + jax.nn.log_sigmoid(pre_forget),
    )
    key_rows = -jnp.expm1(log_forget)
    next_state = (
        jnp.exp(log_forget)[:, :, :, None] * recurrent_state
        + key_rows[:, :, :, None] * value_rows[:, :, None, :]
    )
    query_act = jax.nn.silu(pre_query)
    readout = jnp.einsum("bhk,bhkv->bhv", query_act, next_state, precision=lax.Precision.HIGHEST)
    inv_head = lax.rsqrt(jnp.mean(readout * readout, axis=2, keepdims=True) + epsilon)
    mixed_heads = (readout * inv_head * head_gain * jax.nn.silu(pre_gate)).astype(jnp.bfloat16)
    mixed = gather_blocks(mixed_heads.reshape(own_rows, -1), members)
    mixed = jnp.swapaxes(mixed.reshape(kv, tp, own_rows, -1), 1, 2).reshape(rows, -1)
    out_matrix = out_weight.reshape(-1, out_weight.shape[2])
    projected = jnp.dot(mixed, out_matrix, preferred_element_type=jnp.float32)
    residual = lax.optimization_barrier(
        (tokens.astype(jnp.float32) + projected).astype(jnp.bfloat16)
    )
    normed_mlp = normed_rows(whole_rows(residual, members), mlp_gain)
    hidden = jnp.square(
        jax.nn.relu(jnp.dot(normed_mlp, up_weight, preferred_element_type=jnp.float32))
    ).astype(jnp.bfloat16)
    partial = jnp.dot(hidden, down_weight, preferred_element_type=jnp.float32)
    partial = jnp.swapaxes(partial.reshape(rows, members, -1), 0, 1)
    summed = lax.all_to_all(partial, group, split_axis=0, concat_axis=0, tiled=True).sum(axis=0)
    layer_output = (residual.astype(jnp.float32) + summed).astype(jnp.bfloat16)
    return (layer_output, next_state)


whole = pl.BlockSpec(memory_space=pltpu.VMEM)


def call(body, outs, arrays, flops, limit, scratch=()):
    return pl.pallas_call(
        body,
        out_shape=outs,
        in_specs=[whole] * len(arrays),
        out_specs=jax.tree.map(lambda _: whole, outs),
        scratch_shapes=scratch,
        compiler_params=pltpu.CompilerParams(vmem_limit_bytes=limit),
        cost_estimate=pl.CostEstimate(flops=flops, bytes_accessed=0, transcendentals=0),
    )(*arrays)


def far_step(core):
    return 1 + 2 * core


def placed_blocks(core, near_ref, mid_ref, far_ref, swapped_ref):
    return (
        (0, near_ref),
        (2, mid_ref),
        (far_step(core), far_ref),
        (far_step(1 - core), swapped_ref),
    )


def pair_kernel(own_ref, mate_ref, pair_ref):
    core = lax.axis_index("tp")
    pair_ref[core] = own_ref[...]
    pair_ref[1 - core] = mate_ref[...]


def normed_pieces(pair_refs, gain_ref, rows_ref):
    chip = lax.axis_index("kv")
    cores, _, width = pair_refs[0].shape
    for step, pair_ref in placed_blocks(lax.axis_index("tp"), *pair_refs):
        first = lax.bitwise_xor(chip, step) * (cores * width)
        for core in range(cores):
            place = pl.ds(pl.multiple_of(first + core * width, width), width)
            rows_ref[:, place] = pair_ref[core].astype(jnp.float32)
    rows = rows_ref[...]
    inv_root = lax.rsqrt(jnp.mean(rows * rows, axis=1, keepdims=True) + epsilon)
    return (rows * inv_root * gain_ref[...]).astype(jnp.bfloat16)


def project_kernel(chips, *refs):
    pair_refs, (gain_ref, query_ref, forget_ref, value_ref, gate_ref) = refs[:chips], refs[chips : chips + 5]
    near_ref, mid_ref, far_ref, swap_ref, rows_ref, made_ref = refs[chips + 5 :]
    normed = normed_pieces(pair_refs, gain_ref, rows_ref)
    rows = normed.shape[0]
    heads, chan, _ = query_ref.shape
    lanes = 4 * chan
    for head in range(0, heads, 2):
        weight = jnp.concatenate(
            [
                ref[one]
                for one in (head, head + 1)
                for ref in (query_ref, forget_ref, value_ref, gate_ref)
            ],
            axis=0,
        )
        product = lax.dot_general(
            normed, weight, (((1,), (1,)), ((), ())), preferred_element_type=jnp.float32
        )
        product = product.astype(jnp.bfloat16).astype(jnp.float32)
        made_ref[pl.ds(head, rows, stride=heads), :] = product[:, :lanes]
        made_ref[pl.ds(head + 1, rows, stride=heads), :] = product[:, lanes:]
    chip = lax.axis_index("kv")
    pairs = rows * heads // chips
    for step, sent_ref in placed_blocks(
        lax.axis_index("tp"), near_ref, mid_ref, far_ref, swap_ref
    ):
        first = pl.multiple_of(lax.bitwise_xor(chip, step) * pairs, pairs)
        sent_ref[...] = made_ref[pl.ds(first, pairs), :]


def sigmoid(x):
    return 1.0 / (1.0 + jnp.exp(-x))


def readout_kernel(chips, *refs):
    got_refs, (bound_ref, state_ref, gain_ref) = refs[:chips], refs[chips : chips + 3]
    mixed_ref, key_ref, value_ref, placed_ref = refs[chips + 3 :]
    own_rows, heads, keys, _ = state_ref.shape
    chan = keys // chips
    chip, core = lax.axis_index("kv"), lax.axis_index("tp")
    for step, got_ref in placed_blocks(core, *got_refs):
        block = got_ref[...] if len(got_ref.shape) == 2 else got_ref[core]
        placed_ref[lax.bitwise_xor(chip, step)] = block

    def channels(kind):
        return jnp.concatenate(
            [placed_ref[i][:, kind * chan : (kind + 1) * chan] for i in range(chips)], axis=1
        )

    pre_query, pre_forget, value_rows, pre_gate = (channels(kind) for kind in range(4))
    bound = jnp.concatenate([bound_ref[...]] * own_rows, axis=0)
    gain = jnp.concatenate([gain_ref[...]] * own_rows, axis=0)
    forget = bound + (1.0 - bound) * sigmoid(pre_forget)
    key_rows = (1.0 - bound) * sigmoid(-pre_forget)
    query = pre_query * sigmoid(pre_query)
    new_part = jnp.sum(query * key_rows, axis=1, keepdims=True) * value_rows
    weight = jnp.transpose(query * forget)
    old_parts = []
    for row in range(own_rows):
        for head in range(heads):
            pair = row * heads + head
            old_parts.append(
                jnp.sum(weight[:, pair : pair + 1] * state_ref[row, head], axis=0, keepdims=True)
            )
    readout = jnp.concatenate(old_parts, axis=0) + new_part
    inv_head = lax.rsqrt(jnp.mean(readout * readout, axis=1, keepdims=True) + epsilon)
    mixed = readout * inv_head * gain * (pre_gate * sigmoid(pre_gate))
    mixed_ref[...] = mixed.astype(jnp.bfloat16).astype(jnp.float32)
    key_ref[...] = key_rows
    value_ref[...] = value_rows


def state_kernel(key_ref, value_ref, state_ref, next_ref):
    own_rows, heads, _, _ = state_ref.shape
    key_cols = jnp.transpose(key_ref[...])
    for row in range(own_rows):
        for head in range(heads):
            pair = row * heads + head
            old = state_ref[row, head]
            next_ref[row, head] = old + key_cols[:, pair : pair + 1] * (
                value_ref[pair : pair + 1, :] - old
            )


def stage_kernel(block_ref, staged_ref):
    staged_ref[...] = block_ref[...]


def out_kernel(chips, heads, *refs):
    pair_refs, (tokens_ref, weight_ref, residual_ref, placed_ref) = refs[:chips], refs[chips:]
    cores, pairs, values = pair_refs[0].shape
    own_rows = pairs // heads
    chip = lax.axis_index("kv")
    for step, pair_ref in placed_blocks(lax.axis_index("tp"), *pair_refs):
        first = pl.multiple_of(lax.bitwise_xor(chip, step) * (cores * pairs), cores * pairs)
        placed_ref[pl.ds(first, cores * pairs), :] = pair_ref[...].reshape(-1, values)
    blocks = []
    for core in range(cores):
        for head in range(heads):
            blocks.append(
                jnp.concatenate(
                    [
                        placed_ref[
                            pl.ds(core * pairs + row * heads + head, chips, stride=cores * pairs), :
                        ]
                        for row in range(own_rows)
                    ],
                    axis=0,
                )
            )
    mixed = jnp.concatenate(blocks, axis=1).astype(jnp.bfloat16)
    weight = weight_ref[...].reshape(-1, weight_ref.shape[2])
    projected = jnp.dot(mixed, weight, preferred_element_type=jnp.float32)
    ordered = [
        projected[row * chips + i : row * chips + i + 1]
        for i in range(chips)
        for row in range(own_rows)
    ]
    projected = jnp.concatenate(ordered, axis=0)
    residual_ref[...] = (tokens_ref[...].astype(jnp.float32) + projected).astype(jnp.bfloat16)


def down_part(hidden, down_ref, core, partial_ref):
    width = partial_ref.shape[2]
    chip = lax.axis_index("kv")
    far = lax.bitwise_xor(chip, far_step(core))
    columns = (2 * far, 2 * far + 1, 2 * lax.bitwise_xor(chip, 2) + core, 2 * chip + core)
    for slot, column in enumerate(columns):
        partial_ref[slot] = jnp.dot(
            hidden,
            down_ref[:, pl.ds(pl.multiple_of(column * width, width), width)],
            preferred_element_type=jnp.float32,
        )


def mixer_kernel(chips, *refs):
    pair_refs, (gain_ref, up_ref, down_ref) = refs[:chips], refs[chips : chips + 3]
    hidden_ref, partial_ref, rows_ref = refs[chips + 3 :]
    normed = normed_pieces(pair_refs, gain_ref, rows_ref)
    hidden = jnp.dot(normed, up_ref[...], preferred_element_type=jnp.float32)
    hidden = jnp.square(jnp.maximum(hidden, 0.0)).astype(jnp.bfloat16)
    hidden_ref[...] = hidden
    down_part(hidden, down_ref, 1 - lax.axis_index("tp"), partial_ref)


def own_part_kernel(hidden_ref, down_ref, partial_ref):
    down_part(hidden_ref[...], down_ref, lax.axis_index("tp"), partial_ref)


def chip_sum_kernel(own_ref, mate_ref, far_ref, mid_ref, kept_ref):
    for core in range(2):
        far_ref[core] = (own_ref[core] + mate_ref[core]).astype(jnp.bfloat16)
    mid_ref[...] = (own_ref[2] + mate_ref[2]).astype(jnp.bfloat16)
    kept_ref[...] = own_ref[3] + mate_ref[3]


def last_kernel(residual_ref, kept_ref, mid_ref, far_ref, swapped_ref, state_ref, output_ref):
    del state_ref
    core = lax.axis_index("tp")
    total = kept_ref[...]
    for block in (mid_ref[...], far_ref[core], swapped_ref[core]):
        total = total + block.astype(jnp.float32)
    output_ref[...] = (residual_ref[...].astype(jnp.float32) + total).astype(jnp.bfloat16)


MIB = 1 << 20
COST = (10**11, 10**11, 10**9, 10**9, 10**6, 10**6, 10**9, 10**6, 10**6)


def tiled_local(
    kv,
    tp,
    tokens,
    mix_gain,
    query_weight,
    forget_weight,
    value_weight,
    gate_weight,
    lower_bound,
    recurrent_state,
    head_gain,
    out_weight,
    mlp_gain,
    up_weight,
    down_weight,
):
    rows, width = tokens.shape
    heads, chan, model = query_weight.shape
    own_rows, _, keys, values = recurrent_state.shape
    pairs = own_rows * heads
    shape = jax.ShapeDtypeStruct
    f32, bf16 = jnp.float32, jnp.bfloat16

    def permute(block, steps, swapped=False):
        hops = [
            (k * tp + t, (k ^ steps[t]) * tp + (1 - t if swapped else t))
            for k in range(kv)
            for t in range(tp)
        ]
        return lax.ppermute(block, group, hops)

    def other_core(block):
        return permute(block, (0, 0), True)

    def paired(block, mate, cost):
        return call(pair_kernel, shape((tp,) + block.shape, block.dtype), (block, mate), cost, MIB)

    def crossed(far, mid):
        got_far = permute(far, (1, 3))
        got_mid = permute(mid, (2, 2))
        return got_mid, got_far, permute(got_far, (0, 0), True)

    def gather_pairs(block, staged, cost):
        pair = paired(staged, other_core(block), cost)
        return (pair,) + crossed(pair, pair)

    staged = call(stage_kernel, shape(tokens.shape, bf16), (tokens,), COST[4], MIB)
    near, mid, far, swap = call(
        functools.partial(project_kernel, kv),
        [shape((pairs, 4 * chan), f32)] * kv,
        (
            *gather_pairs(tokens, staged, COST[0]),
            mix_gain.reshape(1, -1),
            query_weight,
            forget_weight,
            value_weight,
            gate_weight,
        ),
        COST[1],
        4 * MIB,
        [pltpu.VMEM((rows, model), f32), pltpu.VMEM((rows * heads, 4 * chan), f32)],
    )
    got = (near,) + crossed(paired(far, other_core(swap), COST[4]), mid)
    mixed, key_rows, value_rows = call(
        functools.partial(readout_kernel, kv),
        [shape((pairs, values), f32), shape((pairs, keys), f32), shape((pairs, values), f32)],
        (*got, lower_bound, recurrent_state, head_gain),
        COST[2],
        4 * MIB,
        [pltpu.VMEM((kv, pairs, 4 * chan), f32)],
    )
    next_state = call(
        state_kernel,
        shape(recurrent_state.shape, f32),
        (key_rows, value_rows, recurrent_state),
        COST[3],
        4 * MIB,
    )
    residual = call(
        functools.partial(out_kernel, kv, heads),
        shape((rows, width), bf16),
        (*gather_pairs(mixed, mixed, COST[4]), staged, out_weight),
        COST[4],
        4 * MIB,
        [pltpu.VMEM((kv * tp * pairs, values), f32)],
    )
    hidden, mate_part = call(
        functools.partial(mixer_kernel, kv),
        [shape((rows, up_weight.shape[1]), bf16), shape((kv, rows, width), f32)],
        (*gather_pairs(residual, residual, COST[4]), mlp_gain.reshape(1, -1), up_weight, down_weight),
        COST[5],
        4 * MIB,
        [pltpu.VMEM((rows, model), f32)],
    )
    own_part = call(
        own_part_kernel, shape((kv, rows, width), f32), (hidden, down_weight), COST[6], 4 * MIB
    )
    far, mid, kept = call(
        chip_sum_kernel,
        [shape((tp, rows, width), bf16), shape((rows, width), bf16), shape((rows, width), f32)],
        (own_part, other_core(mate_part)),
        COST[7],
        MIB,
    )
    sums = crossed(far, mid)
    layer_output = call(
        last_kernel, shape((rows, width), bf16), (residual, kept, *sums, next_state), COST[8], MIB
    )
    return (layer_output, next_state)


def tiles(kv, tp, tokens, query_weight):
    rows, width = tokens.shape
    aligned = rows % 8 == 0 and width % 128 == 0 and query_weight.shape[1] % 32 == 0
    return aligned and tp == 2 and kv == 4


def solution(mesh):
    placed = (
        P("dp", ("kv", "tp")),
        P(),
        P("tp", "kv", None),
        P("tp", "kv", None),
        P("tp", "kv", None),
        P("tp", "kv", None),
        P("tp", None),
        P(("dp", "kv"), "tp", None, None),
        P("tp", None),
        P(None, None, ("kv", "tp")),
        P(),
        P(None, ("kv", "tp")),
        P(("kv", "tp"), None),
    )

    def body(*arrays):
        kv, tp = mesh.shape["kv"], mesh.shape["tp"]
        run = tiled_local if tiles(kv, tp, arrays[0], arrays[2]) else local
        return run(kv, tp, *arrays)

    return jax.shard_map(
        body,
        mesh=mesh,
        in_specs=placed,
        out_specs=(P("dp", ("kv", "tp")), P(("dp", "kv"), "tp", None, None)),
        check_vma=False,
    )
```

```python
import functools

import jax
import jax.numpy as jnp
from jax import lax
from jax.experimental import pallas as pl
from jax.experimental.pallas import tpu as pltpu
from jax.sharding import PartitionSpec as P


epsilon = 1e-06
group = ("kv", "tp")


def gather_blocks(block, members):
    copies = lax.optimization_barrier(jnp.broadcast_to(block[None], (members,) + block.shape))
    return lax.all_to_all(copies, group, split_axis=0, concat_axis=0, tiled=True)


def whole_rows(row_block, members):
    pieces = gather_blocks(row_block, members)
    return jnp.swapaxes(pieces, 0, 1).reshape(row_block.shape[0], -1)


def normed_rows(rows, gain_vector):
    rows = rows.astype(jnp.float32)
    inv_root = lax.rsqrt(jnp.mean(rows * rows, axis=1, keepdims=True) + epsilon)
    return (rows * inv_root * gain_vector).astype(jnp.bfloat16)


def local(
    kv,
    tp,
    tokens,
    mix_gain,
    query_weight,
    forget_weight,
    value_weight,
    gate_weight,
    lower_bound,
    recurrent_state,
    head_gain,
    out_weight,
    mlp_gain,
    up_weight,
    down_weight,
):
    members = kv * tp
    normed = normed_rows(whole_rows(tokens, members), mix_gain)
    local_heads, local_chan, width = query_weight.shape
    rows = normed.shape[0]
    own_rows = rows // kv
    products = [
        lax.dot_general(
            normed,
            weight.reshape(-1, width),
            (((1,), (1,)), ((), ())),
            preferred_element_type=jnp.float32,
        ).astype(jnp.bfloat16)
        for weight in (query_weight, forget_weight, value_weight, gate_weight)
    ]
    product = jnp.stack(products, axis=1).reshape(kv, own_rows * 4 * local_heads, local_chan)
    exchanged = lax.all_to_all(product, "kv", split_axis=0, concat_axis=0, tiled=True)
    channels = jnp.moveaxis(exchanged.reshape(kv, own_rows, 4, local_heads, local_chan), 0, 3)
    channels = channels.reshape(own_rows, 4, local_heads, kv * local_chan).astype(jnp.float32)
    pre_query, pre_forget, value_rows, pre_gate = (channels[:, i] for i in range(4))
    log_forget = jnp.logaddexp(
        jnp.log(lower_bound),
        jnp.log1p(-lower_bound) + jax.nn.log_sigmoid(pre_forget),
    )
    key_rows = -jnp.expm1(log_forget)
    next_state = (
        jnp.exp(log_forget)[:, :, :, None] * recurrent_state
        + key_rows[:, :, :, None] * value_rows[:, :, None, :]
    )
    query_act = jax.nn.silu(pre_query)
    readout = jnp.einsum("bhk,bhkv->bhv", query_act, next_state, precision=lax.Precision.HIGHEST)
    inv_head = lax.rsqrt(jnp.mean(readout * readout, axis=2, keepdims=True) + epsilon)
    mixed_heads = (readout * inv_head * head_gain * jax.nn.silu(pre_gate)).astype(jnp.bfloat16)
    mixed = gather_blocks(mixed_heads.reshape(own_rows, -1), members)
    mixed = jnp.swapaxes(mixed.reshape(kv, tp, own_rows, -1), 1, 2).reshape(rows, -1)
    out_matrix = out_weight.reshape(-1, out_weight.shape[2])
    projected = jnp.dot(mixed, out_matrix, preferred_element_type=jnp.float32)
    residual = lax.optimization_barrier(
        (tokens.astype(jnp.float32) + projected).astype(jnp.bfloat16)
    )
    normed_mlp = normed_rows(whole_rows(residual, members), mlp_gain)
    hidden = jnp.square(
        jax.nn.relu(jnp.dot(normed_mlp, up_weight, preferred_element_type=jnp.float32))
    ).astype(jnp.bfloat16)
    partial = jnp.dot(hidden, down_weight, preferred_element_type=jnp.float32)
    partial = jnp.swapaxes(partial.reshape(rows, members, -1), 0, 1)
    summed = lax.all_to_all(partial, group, split_axis=0, concat_axis=0, tiled=True).sum(axis=0)
    layer_output = (residual.astype(jnp.float32) + summed).astype(jnp.bfloat16)
    return (layer_output, next_state)


whole = pl.BlockSpec(memory_space=pltpu.VMEM)


def call(body, outs, arrays, flops, limit, scratch=()):
    return pl.pallas_call(
        body,
        out_shape=outs,
        in_specs=[whole] * len(arrays),
        out_specs=jax.tree.map(lambda _: whole, outs),
        scratch_shapes=scratch,
        compiler_params=pltpu.CompilerParams(vmem_limit_bytes=limit),
        cost_estimate=pl.CostEstimate(flops=flops, bytes_accessed=0, transcendentals=0),
    )(*arrays)


def far_step(core):
    return 1 + 2 * core


def placed_blocks(core, near_ref, mid_ref, far_ref, swapped_ref):
    return (
        (0, near_ref),
        (2, mid_ref),
        (far_step(core), far_ref),
        (far_step(1 - core), swapped_ref),
    )


def pair_kernel(own_ref, mate_ref, pair_ref):
    core = lax.axis_index("tp")
    pair_ref[core] = own_ref[...]
    pair_ref[1 - core] = mate_ref[...]


def pair_columns(step, width):
    first = lax.bitwise_xor(lax.axis_index("kv"), step) * width
    return pl.ds(pl.multiple_of(first, width), width)


def flat_pair(pair_ref):
    return jnp.concatenate([pair_ref[0], pair_ref[1]], axis=1).astype(jnp.float32)


def scaled_pair(rows, gain_ref, columns):
    return (rows * gain_ref[:, columns]).astype(jnp.bfloat16)


def head_weight(weight_refs, head, columns):
    return jnp.concatenate(
        [ref[one, :, columns] for one in (head, head + 1) for ref in weight_refs], axis=0
    )


def add_projections(steps, gain_ref, weight_refs, start, total_ref):
    heads, chan, _ = weight_refs[0].shape
    lanes = 8 * chan
    blocks = []
    for step, pair_ref in steps:
        rows = flat_pair(pair_ref)
        columns = pair_columns(step, rows.shape[1])
        blocks.append((scaled_pair(rows, gain_ref, columns), columns))
    for head in range(0, heads, 2):
        place = slice(head // 2 * lanes, (head // 2 + 1) * lanes)
        total = start(place)
        for scaled, columns in blocks:
            part = lax.dot_general(
                scaled,
                head_weight(weight_refs, head, columns),
                (((1,), (1,)), ((), ())),
                preferred_element_type=jnp.float32,
            )
            total = part if total is None else total + part
        total_ref[:, place] = total


def early_project_kernel(near_ref, far_ref, gain_ref, *refs):
    weight_refs, total_ref = refs[:4], refs[4]
    steps = ((0, near_ref), (far_step(lax.axis_index("tp")), far_ref))
    add_projections(steps, gain_ref, weight_refs, lambda place: None, total_ref)


def inverse_root(pair_refs):
    squares, width = 0.0, 0
    for pair_ref in pair_refs:
        rows = flat_pair(pair_ref)
        squares = squares + jnp.sum(rows * rows, axis=1, keepdims=True)
        width += rows.shape[1]
    return lax.rsqrt(squares / width + epsilon)


def project_kernel(chips, *refs):
    pair_refs, (early_ref, gain_ref) = refs[:chips], refs[chips : chips + 2]
    weight_refs = refs[chips + 2 : chips + 6]
    near_ref, mid_ref, far_ref, swap_ref, total_ref, made_ref = refs[chips + 6 :]
    core = lax.axis_index("tp")
    steps = ((2, pair_refs[1]), (far_step(1 - core), pair_refs[3]))
    add_projections(steps, gain_ref, weight_refs, lambda place: early_ref[:, place], total_ref)
    heads, chan, _ = weight_refs[0].shape
    rows, lanes = total_ref.shape[0], 4 * chan
    product = total_ref[...] * inverse_root(pair_refs)
    product = product.astype(jnp.bfloat16).astype(jnp.float32)
    for head in range(heads):
        made_ref[pl.ds(head, rows, stride=heads), :] = product[:, head * lanes : (head + 1) * lanes]
    chip = lax.axis_index("kv")
    pairs = rows * heads // chips
    for step, sent_ref in placed_blocks(core, near_ref, mid_ref, far_ref, swap_ref):
        first = pl.multiple_of(lax.bitwise_xor(chip, step) * pairs, pairs)
        sent_ref[...] = made_ref[pl.ds(first, pairs), :]


def sigmoid(x):
    return 1.0 / (1.0 + jnp.exp(-x))


def readout_kernel(chips, *refs):
    got_refs, (bound_ref, state_ref, gain_ref) = refs[:chips], refs[chips : chips + 3]
    mixed_ref, key_ref, value_ref, placed_ref = refs[chips + 3 :]
    own_rows, heads, keys, _ = state_ref.shape
    chan = keys // chips
    chip, core = lax.axis_index("kv"), lax.axis_index("tp")
    for step, got_ref in placed_blocks(core, *got_refs):
        block = got_ref[...] if len(got_ref.shape) == 2 else got_ref[core]
        placed_ref[lax.bitwise_xor(chip, step)] = block

    def channels(kind):
        return jnp.concatenate(
            [placed_ref[i][:, kind * chan : (kind + 1) * chan] for i in range(chips)], axis=1
        )

    pre_query, pre_forget, value_rows, pre_gate = (channels(kind) for kind in range(4))
    bound = jnp.concatenate([bound_ref[...]] * own_rows, axis=0)
    gain = jnp.concatenate([gain_ref[...]] * own_rows, axis=0)
    forget = bound + (1.0 - bound) * sigmoid(pre_forget)
    key_rows = (1.0 - bound) * sigmoid(-pre_forget)
    query = pre_query * sigmoid(pre_query)
    new_part = jnp.sum(query * key_rows, axis=1, keepdims=True) * value_rows
    weight = jnp.transpose(query * forget)
    old_parts = []
    for row in range(own_rows):
        for head in range(heads):
            pair = row * heads + head
            old_parts.append(
                jnp.sum(weight[:, pair : pair + 1] * state_ref[row, head], axis=0, keepdims=True)
            )
    readout = jnp.concatenate(old_parts, axis=0) + new_part
    inv_head = lax.rsqrt(jnp.mean(readout * readout, axis=1, keepdims=True) + epsilon)
    mixed = readout * inv_head * gain * (pre_gate * sigmoid(pre_gate))
    mixed_ref[...] = mixed.astype(jnp.bfloat16).astype(jnp.float32)
    key_ref[...] = key_rows
    value_ref[...] = value_rows


def state_kernel(key_ref, value_ref, state_ref, next_ref, made_ref, done_ref):
    own_rows, heads, _, _ = state_ref.shape
    key_cols = jnp.transpose(key_ref[...])
    copies = []
    for row in range(own_rows):
        for head in range(heads):
            pair = row * heads + head
            old = state_ref[row, head]
            made_ref[pair] = old + key_cols[:, pair : pair + 1] * (
                value_ref[pair : pair + 1, :] - old
            )
            copies.append(
                pltpu.make_async_copy(made_ref.at[pair], next_ref.at[row, head], done_ref.at[pair])
            )
            if pair > 0:
                copies[pair - 1].start()
    copies[-1].start()
    for copy in copies:
        copy.wait()


def stage_kernel(block_ref, staged_ref):
    staged_ref[...] = block_ref[...]


def out_kernel(chips, heads, *refs):
    pair_refs, (tokens_ref, weight_ref, residual_ref, placed_ref) = refs[:chips], refs[chips:]
    cores, pairs, values = pair_refs[0].shape
    own_rows = pairs // heads
    chip = lax.axis_index("kv")
    for step, pair_ref in placed_blocks(lax.axis_index("tp"), *pair_refs):
        first = pl.multiple_of(lax.bitwise_xor(chip, step) * (cores * pairs), cores * pairs)
        placed_ref[pl.ds(first, cores * pairs), :] = pair_ref[...].reshape(-1, values)
    blocks = []
    for core in range(cores):
        for head in range(heads):
            blocks.append(
                jnp.concatenate(
                    [
                        placed_ref[
                            pl.ds(core * pairs + row * heads + head, chips, stride=cores * pairs), :
                        ]
                        for row in range(own_rows)
                    ],
                    axis=0,
                )
            )
    mixed = jnp.concatenate(blocks, axis=1).astype(jnp.bfloat16)
    weight = weight_ref[...].reshape(-1, weight_ref.shape[2])
    projected = jnp.dot(mixed, weight, preferred_element_type=jnp.float32)
    ordered = [
        projected[row * chips + i : row * chips + i + 1]
        for i in range(chips)
        for row in range(own_rows)
    ]
    projected = jnp.concatenate(ordered, axis=0)
    residual_ref[...] = (tokens_ref[...].astype(jnp.float32) + projected).astype(jnp.bfloat16)


def down_part(hidden, down_ref, core, partial_ref):
    width = partial_ref.shape[2]
    chip = lax.axis_index("kv")
    far = lax.bitwise_xor(chip, far_step(core))
    columns = (2 * far, 2 * far + 1, 2 * lax.bitwise_xor(chip, 2) + core, 2 * chip + core)
    for slot, column in enumerate(columns):
        partial_ref[slot] = jnp.dot(
            hidden,
            down_ref[:, pl.ds(pl.multiple_of(column * width, width), width)],
            preferred_element_type=jnp.float32,
        )


def up_part(steps, gain_ref, up_ref, total):
    for step, pair_ref in steps:
        rows = flat_pair(pair_ref)
        columns = pair_columns(step, rows.shape[1])
        part = jnp.dot(
            scaled_pair(rows, gain_ref, columns),
            up_ref[columns, :],
            preferred_element_type=jnp.float32,
        )
        total = part if total is None else total + part
    return total


def early_up_kernel(near_ref, far_ref, gain_ref, up_ref, early_ref):
    steps = ((0, near_ref), (far_step(lax.axis_index("tp")), far_ref))
    early_ref[...] = up_part(steps, gain_ref, up_ref, None)


def mixer_kernel(chips, *refs):
    pair_refs, (early_ref, gain_ref, up_ref, down_ref) = refs[:chips], refs[chips : chips + 4]
    hidden_ref, partial_ref = refs[chips + 4 :]
    core = lax.axis_index("tp")
    steps = ((2, pair_refs[1]), (far_step(1 - core), pair_refs[3]))
    hidden = up_part(steps, gain_ref, up_ref, early_ref[...]) * inverse_root(pair_refs)
    hidden = jnp.square(jnp.maximum(hidden, 0.0)).astype(jnp.bfloat16)
    hidden_ref[...] = hidden
    down_part(hidden, down_ref, 1 - core, partial_ref)


def own_part_kernel(hidden_ref, down_ref, partial_ref):
    down_part(hidden_ref[...], down_ref, lax.axis_index("tp"), partial_ref)


def chip_sum_kernel(own_ref, mate_ref, far_ref, mid_ref, kept_ref):
    for core in range(2):
        far_ref[core] = (own_ref[core] + mate_ref[core]).astype(jnp.bfloat16)
    mid_ref[...] = (own_ref[2] + mate_ref[2]).astype(jnp.bfloat16)
    kept_ref[...] = own_ref[3] + mate_ref[3]


def last_kernel(residual_ref, kept_ref, mid_ref, far_ref, swapped_ref, output_ref):
    core = lax.axis_index("tp")
    total = kept_ref[...]
    for block in (mid_ref[...], far_ref[core], swapped_ref[core]):
        total = total + block.astype(jnp.float32)
    output_ref[...] = (residual_ref[...].astype(jnp.float32) + total).astype(jnp.bfloat16)


MIB = 1 << 20
COST = (10**11, 10**11, 10**9, 10**9, 10**6, 10**6, 10**9, 10**6, 10**6, 10**9, 10**6)


def tiled_local(
    kv,
    tp,
    tokens,
    mix_gain,
    query_weight,
    forget_weight,
    value_weight,
    gate_weight,
    lower_bound,
    recurrent_state,
    head_gain,
    out_weight,
    mlp_gain,
    up_weight,
    down_weight,
):
    rows, width = tokens.shape
    heads, chan, _ = query_weight.shape
    own_rows, _, keys, values = recurrent_state.shape
    pairs = own_rows * heads
    shape = jax.ShapeDtypeStruct
    f32, bf16 = jnp.float32, jnp.bfloat16

    def permute(block, steps, swapped=False):
        hops = [
            (k * tp + t, (k ^ steps[t]) * tp + (1 - t if swapped else t))
            for k in range(kv)
            for t in range(tp)
        ]
        return lax.ppermute(block, group, hops)

    def other_core(block):
        return permute(block, (0, 0), True)

    def paired(block, mate, cost):
        return call(pair_kernel, shape((tp,) + block.shape, block.dtype), (block, mate), cost, MIB)

    def crossed(far, mid):
        got_far = permute(far, (1, 3))
        got_mid = permute(mid, (2, 2))
        return got_mid, got_far, permute(got_far, (0, 0), True)

    def gather_pairs(block, staged, cost):
        pair = paired(staged, other_core(block), cost)
        return (pair,) + crossed(pair, pair)

    staged = call(stage_kernel, shape(tokens.shape, bf16), (tokens,), COST[4], MIB)
    pairs_of_rows = gather_pairs(tokens, staged, COST[0])
    mix_row = mix_gain.reshape(1, -1)
    projections = (query_weight, forget_weight, value_weight, gate_weight)
    early = call(
        early_project_kernel,
        shape((rows, 4 * heads * chan), f32),
        (pairs_of_rows[0], pairs_of_rows[2], mix_row, *projections),
        COST[9],
        14 * MIB,
    )
    near, mid, far, swap = call(
        functools.partial(project_kernel, kv),
        [shape((pairs, 4 * chan), f32)] * kv,
        (*pairs_of_rows, early, mix_row, *projections),
        COST[1],
        14 * MIB,
        [pltpu.VMEM((rows, 4 * heads * chan), f32), pltpu.VMEM((rows * heads, 4 * chan), f32)],
    )
    got = (near,) + crossed(paired(far, other_core(swap), COST[4]), mid)
    mixed, key_rows, value_rows = call(
        functools.partial(readout_kernel, kv),
        [shape((pairs, values), f32), shape((pairs, keys), f32), shape((pairs, values), f32)],
        (*got, lower_bound, recurrent_state, head_gain),
        COST[2],
        14 * MIB,
        [pltpu.VMEM((kv, pairs, 4 * chan), f32)],
    )
    next_state = pl.pallas_call(
        state_kernel,
        out_shape=shape(recurrent_state.shape, f32),
        in_specs=[whole] * 3,
        out_specs=pl.BlockSpec(memory_space=pl.ANY),
        scratch_shapes=[pltpu.VMEM((pairs, keys, values), f32), pltpu.SemaphoreType.DMA((pairs,))],
        compiler_params=pltpu.CompilerParams(vmem_limit_bytes=6 * MIB),
        cost_estimate=pl.CostEstimate(flops=COST[3], bytes_accessed=0, transcendentals=0),
    )(key_rows, value_rows, recurrent_state)
    residual = call(
        functools.partial(out_kernel, kv, heads),
        shape((rows, width), bf16),
        (*gather_pairs(mixed, mixed, COST[4]), tokens, out_weight),
        COST[4],
        14 * MIB,
        [pltpu.VMEM((kv * tp * pairs, values), f32)],
    )
    pairs_of_rows = gather_pairs(residual, residual, COST[4])
    mlp_row = mlp_gain.reshape(1, -1)
    early = call(
        early_up_kernel,
        shape((rows, up_weight.shape[1]), f32),
        (pairs_of_rows[0], pairs_of_rows[2], mlp_row, up_weight),
        COST[10],
        14 * MIB,
    )
    hidden, mate_part = call(
        functools.partial(mixer_kernel, kv),
        [shape((rows, up_weight.shape[1]), bf16), shape((kv, rows, width), f32)],
        (*pairs_of_rows, early, mlp_row, up_weight, down_weight),
        COST[5],
        14 * MIB,
    )
    own_part = call(
        own_part_kernel, shape((kv, rows, width), f32), (hidden, down_weight), COST[6], 14 * MIB
    )
    far, mid, kept = call(
        chip_sum_kernel,
        [shape((tp, rows, width), bf16), shape((rows, width), bf16), shape((rows, width), f32)],
        (own_part, other_core(mate_part)),
        COST[7],
        MIB,
    )
    sums = crossed(far, mid)
    layer_output = call(
        last_kernel, shape((rows, width), bf16), (residual, kept, *sums), COST[8], MIB
    )
    return (layer_output, next_state)


def tiles(kv, tp, tokens, query_weight):
    rows, width = tokens.shape
    aligned = rows % 8 == 0 and width % 128 == 0 and query_weight.shape[1] % 32 == 0
    return aligned and tp == 2 and kv == 4


def solution(mesh):
    placed = (
        P("dp", ("kv", "tp")),
        P(),
        P("tp", "kv", None),
        P("tp", "kv", None),
        P("tp", "kv", None),
        P("tp", "kv", None),
        P("tp", None),
        P(("dp", "kv"), "tp", None, None),
        P("tp", None),
        P(None, None, ("kv", "tp")),
        P(),
        P(None, ("kv", "tp")),
        P(("kv", "tp"), None),
    )

    def body(*arrays):
        kv, tp = mesh.shape["kv"], mesh.shape["tp"]
        run = tiled_local if tiles(kv, tp, arrays[0], arrays[2]) else local
        return run(kv, tp, *arrays)

    return jax.shard_map(
        body,
        mesh=mesh,
        in_specs=placed,
        out_specs=(P("dp", ("kv", "tp")), P(("dp", "kv"), "tp", None, None)),
        check_vma=False,
    )
```

```python
import functools

import jax
import jax.numpy as jnp
from jax import lax
from jax.experimental import pallas as pl
from jax.experimental.pallas import tpu as pltpu
from jax.sharding import PartitionSpec as P


epsilon = 1e-06
group = ("kv", "tp")


def gather_blocks(block, members):
    copies = lax.optimization_barrier(jnp.broadcast_to(block[None], (members,) + block.shape))
    return lax.all_to_all(copies, group, split_axis=0, concat_axis=0, tiled=True)


def whole_rows(row_block, members):
    pieces = gather_blocks(row_block, members)
    return jnp.swapaxes(pieces, 0, 1).reshape(row_block.shape[0], -1)


def normed_rows(rows, gain_vector):
    rows = rows.astype(jnp.float32)
    inv_root = lax.rsqrt(jnp.mean(rows * rows, axis=1, keepdims=True) + epsilon)
    return (rows * inv_root * gain_vector).astype(jnp.bfloat16)


def local(
    kv,
    tp,
    tokens,
    mix_gain,
    query_weight,
    forget_weight,
    value_weight,
    gate_weight,
    lower_bound,
    recurrent_state,
    head_gain,
    out_weight,
    mlp_gain,
    up_weight,
    down_weight,
):
    members = kv * tp
    normed = normed_rows(whole_rows(tokens, members), mix_gain)
    local_heads, local_chan, width = query_weight.shape
    rows = normed.shape[0]
    own_rows = rows // kv
    products = [
        lax.dot_general(
            normed,
            weight.reshape(-1, width),
            (((1,), (1,)), ((), ())),
            preferred_element_type=jnp.float32,
        ).astype(jnp.bfloat16)
        for weight in (query_weight, forget_weight, value_weight, gate_weight)
    ]
    product = jnp.stack(products, axis=1).reshape(kv, own_rows * 4 * local_heads, local_chan)
    exchanged = lax.all_to_all(product, "kv", split_axis=0, concat_axis=0, tiled=True)
    channels = jnp.moveaxis(exchanged.reshape(kv, own_rows, 4, local_heads, local_chan), 0, 3)
    channels = channels.reshape(own_rows, 4, local_heads, kv * local_chan).astype(jnp.float32)
    pre_query, pre_forget, value_rows, pre_gate = (channels[:, i] for i in range(4))
    log_forget = jnp.logaddexp(
        jnp.log(lower_bound),
        jnp.log1p(-lower_bound) + jax.nn.log_sigmoid(pre_forget),
    )
    key_rows = -jnp.expm1(log_forget)
    next_state = (
        jnp.exp(log_forget)[:, :, :, None] * recurrent_state
        + key_rows[:, :, :, None] * value_rows[:, :, None, :]
    )
    query_act = jax.nn.silu(pre_query)
    readout = jnp.einsum("bhk,bhkv->bhv", query_act, next_state, precision=lax.Precision.HIGHEST)
    inv_head = lax.rsqrt(jnp.mean(readout * readout, axis=2, keepdims=True) + epsilon)
    mixed_heads = (readout * inv_head * head_gain * jax.nn.silu(pre_gate)).astype(jnp.bfloat16)
    mixed = gather_blocks(mixed_heads.reshape(own_rows, -1), members)
    mixed = jnp.swapaxes(mixed.reshape(kv, tp, own_rows, -1), 1, 2).reshape(rows, -1)
    out_matrix = out_weight.reshape(-1, out_weight.shape[2])
    projected = jnp.dot(mixed, out_matrix, preferred_element_type=jnp.float32)
    residual = lax.optimization_barrier(
        (tokens.astype(jnp.float32) + projected).astype(jnp.bfloat16)
    )
    normed_mlp = normed_rows(whole_rows(residual, members), mlp_gain)
    hidden = jnp.square(
        jax.nn.relu(jnp.dot(normed_mlp, up_weight, preferred_element_type=jnp.float32))
    ).astype(jnp.bfloat16)
    partial = jnp.dot(hidden, down_weight, preferred_element_type=jnp.float32)
    partial = jnp.swapaxes(partial.reshape(rows, members, -1), 0, 1)
    summed = lax.all_to_all(partial, group, split_axis=0, concat_axis=0, tiled=True).sum(axis=0)
    layer_output = (residual.astype(jnp.float32) + summed).astype(jnp.bfloat16)
    return (layer_output, next_state)


whole = pl.BlockSpec(memory_space=pltpu.VMEM)


def call(body, outs, arrays, flops, limit, scratch=()):
    return pl.pallas_call(
        body,
        out_shape=outs,
        in_specs=[whole] * len(arrays),
        out_specs=jax.tree.map(lambda _: whole, outs),
        scratch_shapes=scratch,
        compiler_params=pltpu.CompilerParams(vmem_limit_bytes=limit),
        cost_estimate=pl.CostEstimate(flops=flops, bytes_accessed=0, transcendentals=0),
    )(*arrays)


def far_step(core):
    return 1 + 2 * core


def placed_blocks(core, near_ref, mid_ref, far_ref, swapped_ref):
    return (
        (0, near_ref),
        (2, mid_ref),
        (far_step(core), far_ref),
        (far_step(1 - core), swapped_ref),
    )


def pair_kernel(own_ref, mate_ref, pair_ref):
    core = lax.axis_index("tp")
    pair_ref[core] = own_ref[...]
    pair_ref[1 - core] = mate_ref[...]


def pair_columns(step, width):
    first = lax.bitwise_xor(lax.axis_index("kv"), step) * width
    return pl.ds(pl.multiple_of(first, width), width)


def flat_pair(pair_ref):
    return jnp.concatenate([pair_ref[0], pair_ref[1]], axis=1).astype(jnp.float32)


def split_pair(pair_ref, gain_ref, columns):
    scaled = flat_pair(pair_ref) * gain_ref[:, columns]
    high = scaled.astype(jnp.bfloat16)
    low = (scaled - high.astype(jnp.float32)).astype(jnp.bfloat16)
    return jnp.concatenate([high, low], axis=0)


def normed_pair(pair_ref, gain_ref, columns, inv_root):
    return (flat_pair(pair_ref) * inv_root * gain_ref[:, columns]).astype(jnp.bfloat16)


def joined(product):
    half = product.shape[0] // 2
    return product[:half] + product[half:]


def head_weight(weight_refs, head, columns):
    return jnp.concatenate(
        [ref[one, :, columns] for one in (head, head + 1) for ref in weight_refs], axis=0
    )


def project_blocks(blocks, weight_refs, finish):
    heads, chan, _ = weight_refs[0].shape
    lanes = 8 * chan
    for head in range(0, heads, 2):
        total = None
        for rows, columns in blocks:
            part = lax.dot_general(
                rows,
                head_weight(weight_refs, head, columns),
                (((1,), (1,)), ((), ())),
                preferred_element_type=jnp.float32,
            )
            total = part if total is None else total + part
        finish(slice(head // 2 * lanes, (head // 2 + 1) * lanes), total)


def near_step():
    return 0


def other_step():
    return far_step(lax.axis_index("tp"))


def late_steps(pair_refs):
    return ((2, pair_refs[1]), (far_step(1 - lax.axis_index("tp")), pair_refs[3]))


def split_blocks(steps, gain_ref):
    blocks = []
    for step, pair_ref in steps:
        columns = pair_columns(step, 2 * pair_ref.shape[2])
        blocks.append((split_pair(pair_ref, gain_ref, columns), columns))
    return blocks


def normed_blocks(steps, gain_ref, inv_root):
    blocks = []
    for step, pair_ref in steps:
        columns = pair_columns(step, 2 * pair_ref.shape[2])
        blocks.append((normed_pair(pair_ref, gain_ref, columns, inv_root), columns))
    return blocks


def early_project_kernel(step, pair_ref, gain_ref, *refs):
    weight_refs, before_refs, total_ref = refs[:4], refs[4:-1], refs[-1]

    def finish(place, total):
        total = joined(total)
        for ref in before_refs:
            total = total + ref[:, place]
        total_ref[:, place] = total

    project_blocks(split_blocks(((step(), pair_ref),), gain_ref), weight_refs, finish)


def inverse_root(pair_refs):
    squares, width = 0.0, 0
    for pair_ref in pair_refs:
        rows = flat_pair(pair_ref)
        squares = squares + jnp.sum(rows * rows, axis=1, keepdims=True)
        width += rows.shape[1]
    return lax.rsqrt(squares / width + epsilon)


def project_kernel(chips, *refs):
    pair_refs, (early_ref, gain_ref) = refs[:chips], refs[chips : chips + 2]
    weight_refs = refs[chips + 2 : chips + 6]
    near_ref, mid_ref, far_ref, swap_ref, total_ref, made_ref = refs[chips + 6 :]
    core = lax.axis_index("tp")
    inv_root = inverse_root(pair_refs)

    def finish(place, total):
        total_ref[:, place] = early_ref[:, place] * inv_root + total

    project_blocks(normed_blocks(late_steps(pair_refs), gain_ref, inv_root), weight_refs, finish)
    heads, chan, _ = weight_refs[0].shape
    rows, lanes = total_ref.shape[0], 4 * chan
    product = total_ref[...].astype(jnp.bfloat16).astype(jnp.float32)
    for head in range(heads):
        made_ref[pl.ds(head, rows, stride=heads), :] = product[:, head * lanes : (head + 1) * lanes]
    chip = lax.axis_index("kv")
    pairs = rows * heads // chips
    for step, sent_ref in placed_blocks(core, near_ref, mid_ref, far_ref, swap_ref):
        first = pl.multiple_of(lax.bitwise_xor(chip, step) * pairs, pairs)
        sent_ref[...] = made_ref[pl.ds(first, pairs), :]


def sigmoid(x):
    return 1.0 / (1.0 + jnp.exp(-x))


def readout_kernel(chips, *refs):
    got_refs, (bound_ref, state_ref, gain_ref) = refs[:chips], refs[chips : chips + 3]
    mixed_ref, key_ref, value_ref, placed_ref = refs[chips + 3 :]
    own_rows, heads, keys, _ = state_ref.shape
    chan = keys // chips
    chip, core = lax.axis_index("kv"), lax.axis_index("tp")
    for step, got_ref in placed_blocks(core, *got_refs):
        block = got_ref[...] if len(got_ref.shape) == 2 else got_ref[core]
        placed_ref[lax.bitwise_xor(chip, step)] = block

    def channels(kind):
        return jnp.concatenate(
            [placed_ref[i][:, kind * chan : (kind + 1) * chan] for i in range(chips)], axis=1
        )

    pre_query, pre_forget, value_rows, pre_gate = (channels(kind) for kind in range(4))
    bound = jnp.concatenate([bound_ref[...]] * own_rows, axis=0)
    gain = jnp.concatenate([gain_ref[...]] * own_rows, axis=0)
    forget = bound + (1.0 - bound) * sigmoid(pre_forget)
    key_rows = (1.0 - bound) * sigmoid(-pre_forget)
    query = pre_query * sigmoid(pre_query)
    new_part = jnp.sum(query * key_rows, axis=1, keepdims=True) * value_rows
    weight = jnp.transpose(query * forget)
    old_parts = []
    for row in range(own_rows):
        for head in range(heads):
            pair = row * heads + head
            old_parts.append(
                jnp.sum(weight[:, pair : pair + 1] * state_ref[row, head], axis=0, keepdims=True)
            )
    readout = jnp.concatenate(old_parts, axis=0) + new_part
    inv_head = lax.rsqrt(jnp.mean(readout * readout, axis=1, keepdims=True) + epsilon)
    mixed = readout * inv_head * gain * (pre_gate * sigmoid(pre_gate))
    mixed_ref[...] = mixed.astype(jnp.bfloat16).astype(jnp.float32)
    key_ref[...] = key_rows
    value_ref[...] = value_rows


def state_kernel(key_ref, value_ref, state_ref, next_ref):
    own_rows, heads, _, _ = state_ref.shape
    key_cols = jnp.transpose(key_ref[...])
    for row in range(own_rows):
        for head in range(heads):
            pair = row * heads + head
            old = state_ref[row, head]
            next_ref[row, head] = old + key_cols[:, pair : pair + 1] * (
                value_ref[pair : pair + 1, :] - old
            )


def copy_out_kernel(made_ref, next_ref, done_ref):
    copy = pltpu.make_async_copy(made_ref, next_ref, done_ref)
    copy.start()
    copy.wait()


def stage_kernel(block_ref, staged_ref):
    staged_ref[...] = block_ref[...]


def out_kernel(chips, heads, *refs):
    pair_refs, (tokens_ref, weight_ref, residual_ref, placed_ref) = refs[:chips], refs[chips:]
    cores, pairs, values = pair_refs[0].shape
    own_rows = pairs // heads
    chip = lax.axis_index("kv")
    for step, pair_ref in placed_blocks(lax.axis_index("tp"), *pair_refs):
        first = pl.multiple_of(lax.bitwise_xor(chip, step) * (cores * pairs), cores * pairs)
        placed_ref[pl.ds(first, cores * pairs), :] = pair_ref[...].reshape(-1, values)
    blocks = []
    for core in range(cores):
        for head in range(heads):
            blocks.append(
                jnp.concatenate(
                    [
                        placed_ref[
                            pl.ds(core * pairs + row * heads + head, chips, stride=cores * pairs), :
                        ]
                        for row in range(own_rows)
                    ],
                    axis=0,
                )
            )
    mixed = jnp.concatenate(blocks, axis=1).astype(jnp.bfloat16)
    weight = weight_ref[...].reshape(-1, weight_ref.shape[2])
    projected = jnp.dot(mixed, weight, preferred_element_type=jnp.float32)
    ordered = [
        projected[row * chips + i : row * chips + i + 1]
        for i in range(chips)
        for row in range(own_rows)
    ]
    projected = jnp.concatenate(ordered, axis=0)
    residual_ref[...] = (tokens_ref[...].astype(jnp.float32) + projected).astype(jnp.bfloat16)


def down_part(hidden, down_ref, core, partial_ref):
    width = partial_ref.shape[2]
    chip = lax.axis_index("kv")
    far = lax.bitwise_xor(chip, far_step(core))
    columns = (2 * far, 2 * far + 1, 2 * lax.bitwise_xor(chip, 2) + core, 2 * chip + core)
    for slot, column in enumerate(columns):
        partial_ref[slot] = jnp.dot(
            hidden,
            down_ref[:, pl.ds(pl.multiple_of(column * width, width), width)],
            preferred_element_type=jnp.float32,
        )


def up_blocks(blocks, up_ref):
    total = None
    for rows, columns in blocks:
        part = jnp.dot(rows, up_ref[columns, :], preferred_element_type=jnp.float32)
        total = part if total is None else total + part
    return total


def early_up_kernel(step, pair_ref, gain_ref, up_ref, down_ref, *refs):
    del down_ref
    total = joined(up_blocks(split_blocks(((step(), pair_ref),), gain_ref), up_ref))
    for ref in refs[:-1]:
        total = total + ref[...]
    refs[-1][...] = total


def mixer_kernel(chips, *refs):
    pair_refs, (early_ref, gain_ref, up_ref, down_ref) = refs[:chips], refs[chips : chips + 4]
    hidden_ref, partial_ref = refs[chips + 4 :]
    inv_root = inverse_root(pair_refs)
    late = up_blocks(normed_blocks(late_steps(pair_refs), gain_ref, inv_root), up_ref)
    hidden = early_ref[...] * inv_root + late
    hidden = jnp.square(jnp.maximum(hidden, 0.0)).astype(jnp.bfloat16)
    hidden_ref[...] = hidden
    down_part(hidden, down_ref, 1 - lax.axis_index("tp"), partial_ref)


def own_part_kernel(hidden_ref, down_ref, partial_ref):
    down_part(hidden_ref[...], down_ref, lax.axis_index("tp"), partial_ref)


def chip_sum_kernel(own_ref, mate_ref, far_ref, mid_ref, kept_ref):
    for core in range(2):
        far_ref[core] = (own_ref[core] + mate_ref[core]).astype(jnp.bfloat16)
    mid_ref[...] = (own_ref[2] + mate_ref[2]).astype(jnp.bfloat16)
    kept_ref[...] = own_ref[3] + mate_ref[3]


def last_kernel(residual_ref, kept_ref, mid_ref, far_ref, swapped_ref, output_ref):
    core = lax.axis_index("tp")
    total = kept_ref[...]
    for block in (mid_ref[...], far_ref[core], swapped_ref[core]):
        total = total + block.astype(jnp.float32)
    output_ref[...] = (residual_ref[...].astype(jnp.float32) + total).astype(jnp.bfloat16)


MIB = 1 << 20
COST = (10**11, 10**11, 10**9, 10**9, 10**6, 10**6, 10**9, 10**6, 10**6, 10**9, 10**6)


def tiled_local(
    kv,
    tp,
    tokens,
    mix_gain,
    query_weight,
    forget_weight,
    value_weight,
    gate_weight,
    lower_bound,
    recurrent_state,
    head_gain,
    out_weight,
    mlp_gain,
    up_weight,
    down_weight,
):
    rows, width = tokens.shape
    heads, chan, _ = query_weight.shape
    own_rows, _, keys, values = recurrent_state.shape
    pairs = own_rows * heads
    shape = jax.ShapeDtypeStruct
    f32, bf16 = jnp.float32, jnp.bfloat16

    def permute(block, steps, swapped=False):
        hops = [
            (k * tp + t, (k ^ steps[t]) * tp + (1 - t if swapped else t))
            for k in range(kv)
            for t in range(tp)
        ]
        return lax.ppermute(block, group, hops)

    def other_core(block):
        return permute(block, (0, 0), True)

    def paired(block, mate, cost):
        return call(pair_kernel, shape((tp,) + block.shape, block.dtype), (block, mate), cost, MIB)

    def crossed(far, mid):
        got_far = permute(far, (1, 3))
        got_mid = permute(mid, (2, 2))
        return got_mid, got_far, permute(got_far, (0, 0), True)

    def gather_pairs(block, staged, cost):
        pair = paired(staged, other_core(block), cost)
        return (pair,) + crossed(pair, pair)

    def early_parts(kernel, got, operands, columns, cost):
        total = ()
        for place, step in ((0, near_step), (2, other_step)):
            part = call(
                functools.partial(kernel, step),
                shape((rows, columns), f32),
                (got[place], *operands, *total),
                cost,
                14 * MIB,
            )
            total = (part,)
        return total[0]

    staged = call(stage_kernel, shape(tokens.shape, bf16), (tokens,), COST[4], MIB)
    pairs_of_rows = gather_pairs(tokens, staged, COST[0])
    mix_row = mix_gain.reshape(1, -1)
    projections = (query_weight, forget_weight, value_weight, gate_weight)
    early = early_parts(
        early_project_kernel, pairs_of_rows, (mix_row, *projections), 4 * heads * chan, COST[9]
    )
    near, mid, far, swap = call(
        functools.partial(project_kernel, kv),
        [shape((pairs, 4 * chan), f32)] * kv,
        (*pairs_of_rows, early, mix_row, *projections),
        COST[1],
        14 * MIB,
        [pltpu.VMEM((rows, 4 * heads * chan), f32), pltpu.VMEM((rows * heads, 4 * chan), f32)],
    )
    got = (near,) + crossed(paired(far, other_core(swap), COST[4]), mid)
    mixed, key_rows, value_rows = call(
        functools.partial(readout_kernel, kv),
        [shape((pairs, values), f32), shape((pairs, keys), f32), shape((pairs, values), f32)],
        (*got, lower_bound, recurrent_state, head_gain),
        COST[2],
        14 * MIB,
        [pltpu.VMEM((kv, pairs, 4 * chan), f32)],
    )
    next_state = call(
        state_kernel,
        pltpu.VMEM(recurrent_state.shape, f32),
        (key_rows, value_rows, recurrent_state),
        COST[3],
        4 * MIB,
    )
    next_state = pl.pallas_call(
        copy_out_kernel,
        out_shape=shape(recurrent_state.shape, f32),
        in_specs=[whole],
        out_specs=pl.BlockSpec(memory_space=pl.ANY),
        scratch_shapes=[pltpu.SemaphoreType.DMA],
        compiler_params=pltpu.CompilerParams(vmem_limit_bytes=MIB),
        cost_estimate=pl.CostEstimate(flops=COST[3], bytes_accessed=0, transcendentals=0),
    )(next_state)
    residual = call(
        functools.partial(out_kernel, kv, heads),
        shape((rows, width), bf16),
        (*gather_pairs(mixed, mixed, COST[4]), tokens, out_weight),
        COST[4],
        14 * MIB,
        [pltpu.VMEM((kv * tp * pairs, values), f32)],
    )
    pairs_of_rows = gather_pairs(residual, residual, COST[4])
    mlp_row = mlp_gain.reshape(1, -1)
    early = early_parts(
        early_up_kernel, pairs_of_rows, (mlp_row, up_weight, down_weight), up_weight.shape[1], COST[10]
    )
    hidden, mate_part = call(
        functools.partial(mixer_kernel, kv),
        [shape((rows, up_weight.shape[1]), bf16), shape((kv, rows, width), f32)],
        (*pairs_of_rows, early, mlp_row, up_weight, down_weight),
        COST[5],
        14 * MIB,
    )
    own_part = call(
        own_part_kernel, shape((kv, rows, width), f32), (hidden, down_weight), COST[6], 14 * MIB
    )
    far, mid, kept = call(
        chip_sum_kernel,
        [shape((tp, rows, width), bf16), shape((rows, width), bf16), shape((rows, width), f32)],
        (own_part, other_core(mate_part)),
        COST[7],
        MIB,
    )
    sums = crossed(far, mid)
    layer_output = call(
        last_kernel, shape((rows, width), bf16), (residual, kept, *sums), COST[8], MIB
    )
    return (layer_output, next_state)


def tiles(kv, tp, tokens, query_weight):
    rows, width = tokens.shape
    aligned = rows % 8 == 0 and width % 128 == 0 and query_weight.shape[1] % 32 == 0
    return aligned and tp == 2 and kv == 4


def solution(mesh):
    placed = (
        P("dp", ("kv", "tp")),
        P(),
        P("tp", "kv", None),
        P("tp", "kv", None),
        P("tp", "kv", None),
        P("tp", "kv", None),
        P("tp", None),
        P(("dp", "kv"), "tp", None, None),
        P("tp", None),
        P(None, None, ("kv", "tp")),
        P(),
        P(None, ("kv", "tp")),
        P(("kv", "tp"), None),
    )

    def body(*arrays):
        kv, tp = mesh.shape["kv"], mesh.shape["tp"]
        run = tiled_local if tiles(kv, tp, arrays[0], arrays[2]) else local
        return run(kv, tp, *arrays)

    return jax.shard_map(
        body,
        mesh=mesh,
        in_specs=placed,
        out_specs=(P("dp", ("kv", "tp")), P(("dp", "kv"), "tp", None, None)),
        check_vma=False,
    )
```

```python
import functools

import jax
import jax.numpy as jnp
from jax import lax
from jax.experimental import pallas as pl
from jax.experimental.pallas import tpu as pltpu
from jax.sharding import PartitionSpec as P


epsilon = 1e-06
group = ("kv", "tp")


def gather_blocks(block, members):
    copies = lax.optimization_barrier(jnp.broadcast_to(block[None], (members,) + block.shape))
    return lax.all_to_all(copies, group, split_axis=0, concat_axis=0, tiled=True)


def whole_rows(row_block, members):
    pieces = gather_blocks(row_block, members)
    return jnp.swapaxes(pieces, 0, 1).reshape(row_block.shape[0], -1)


def normed_rows(rows, gain_vector):
    rows = rows.astype(jnp.float32)
    inv_root = lax.rsqrt(jnp.mean(rows * rows, axis=1, keepdims=True) + epsilon)
    return (rows * inv_root * gain_vector).astype(jnp.bfloat16)


def local(
    kv,
    tp,
    tokens,
    mix_gain,
    query_weight,
    forget_weight,
    value_weight,
    gate_weight,
    lower_bound,
    recurrent_state,
    head_gain,
    out_weight,
    mlp_gain,
    up_weight,
    down_weight,
):
    members = kv * tp
    normed = normed_rows(whole_rows(tokens, members), mix_gain)
    local_heads, local_chan, width = query_weight.shape
    rows = normed.shape[0]
    own_rows = rows // kv
    products = [
        lax.dot_general(
            normed,
            weight.reshape(-1, width),
            (((1,), (1,)), ((), ())),
            preferred_element_type=jnp.float32,
        ).astype(jnp.bfloat16)
        for weight in (query_weight, forget_weight, value_weight, gate_weight)
    ]
    product = jnp.stack(products, axis=1).reshape(kv, own_rows * 4 * local_heads, local_chan)
    exchanged = lax.all_to_all(product, "kv", split_axis=0, concat_axis=0, tiled=True)
    channels = jnp.moveaxis(exchanged.reshape(kv, own_rows, 4, local_heads, local_chan), 0, 3)
    channels = channels.reshape(own_rows, 4, local_heads, kv * local_chan).astype(jnp.float32)
    pre_query, pre_forget, value_rows, pre_gate = (channels[:, i] for i in range(4))
    log_forget = jnp.logaddexp(
        jnp.log(lower_bound),
        jnp.log1p(-lower_bound) + jax.nn.log_sigmoid(pre_forget),
    )
    key_rows = -jnp.expm1(log_forget)
    next_state = (
        jnp.exp(log_forget)[:, :, :, None] * recurrent_state
        + key_rows[:, :, :, None] * value_rows[:, :, None, :]
    )
    query_act = jax.nn.silu(pre_query)
    readout = jnp.einsum("bhk,bhkv->bhv", query_act, next_state, precision=lax.Precision.HIGHEST)
    inv_head = lax.rsqrt(jnp.mean(readout * readout, axis=2, keepdims=True) + epsilon)
    mixed_heads = (readout * inv_head * head_gain * jax.nn.silu(pre_gate)).astype(jnp.bfloat16)
    mixed = gather_blocks(mixed_heads.reshape(own_rows, -1), members)
    mixed = jnp.swapaxes(mixed.reshape(kv, tp, own_rows, -1), 1, 2).reshape(rows, -1)
    out_matrix = out_weight.reshape(-1, out_weight.shape[2])
    projected = jnp.dot(mixed, out_matrix, preferred_element_type=jnp.float32)
    residual = lax.optimization_barrier(
        (tokens.astype(jnp.float32) + projected).astype(jnp.bfloat16)
    )
    normed_mlp = normed_rows(whole_rows(residual, members), mlp_gain)
    hidden = jnp.square(
        jax.nn.relu(jnp.dot(normed_mlp, up_weight, preferred_element_type=jnp.float32))
    ).astype(jnp.bfloat16)
    partial = jnp.dot(hidden, down_weight, preferred_element_type=jnp.float32)
    partial = jnp.swapaxes(partial.reshape(rows, members, -1), 0, 1)
    summed = lax.all_to_all(partial, group, split_axis=0, concat_axis=0, tiled=True).sum(axis=0)
    layer_output = (residual.astype(jnp.float32) + summed).astype(jnp.bfloat16)
    return (layer_output, next_state)


whole = pl.BlockSpec(memory_space=pltpu.VMEM)


def call(body, outs, arrays, flops, limit, scratch=()):
    return pl.pallas_call(
        body,
        out_shape=outs,
        in_specs=[whole] * len(arrays),
        out_specs=jax.tree.map(lambda _: whole, outs),
        scratch_shapes=scratch,
        compiler_params=pltpu.CompilerParams(vmem_limit_bytes=limit),
        cost_estimate=pl.CostEstimate(flops=flops, bytes_accessed=0, transcendentals=0),
    )(*arrays)


def far_step(core):
    return 1 + 2 * core


def placed_blocks(core, near_ref, mid_ref, far_ref, swapped_ref):
    return (
        (0, near_ref),
        (2, mid_ref),
        (far_step(core), far_ref),
        (far_step(1 - core), swapped_ref),
    )


def pair_kernel(own_ref, mate_ref, pair_ref):
    core = lax.axis_index("tp")
    pair_ref[core] = own_ref[...]
    pair_ref[1 - core] = mate_ref[...]


def pair_columns(step, width):
    first = lax.bitwise_xor(lax.axis_index("kv"), step) * width
    return pl.ds(pl.multiple_of(first, width), width)


def flat_pair(pair_ref):
    return jnp.concatenate([pair_ref[0], pair_ref[1]], axis=1).astype(jnp.float32)


def split_pair(pair_ref, gain_ref, columns):
    scaled = flat_pair(pair_ref) * gain_ref[:, columns]
    high = scaled.astype(jnp.bfloat16)
    low = (scaled - high.astype(jnp.float32)).astype(jnp.bfloat16)
    return jnp.concatenate([high, low], axis=0)


def normed_pair(pair_ref, gain_ref, columns, inv_root):
    return (flat_pair(pair_ref) * inv_root * gain_ref[:, columns]).astype(jnp.bfloat16)


def joined(product):
    half = product.shape[0] // 2
    return product[:half] + product[half:]


def head_weight(weight_refs, head, columns):
    return jnp.concatenate(
        [ref[one, :, columns] for one in (head, head + 1) for ref in weight_refs], axis=0
    )


def project_blocks(blocks, weight_refs, finish):
    heads, chan, _ = weight_refs[0].shape
    lanes = 8 * chan
    for head in range(0, heads, 2):
        total = None
        for rows, columns in blocks:
            part = lax.dot_general(
                rows,
                head_weight(weight_refs, head, columns),
                (((1,), (1,)), ((), ())),
                preferred_element_type=jnp.float32,
            )
            total = part if total is None else total + part
        finish(slice(head // 2 * lanes, (head // 2 + 1) * lanes), total)


def near_step():
    return 0


def other_step():
    return far_step(lax.axis_index("tp"))


def late_steps(pair_refs):
    return ((2, pair_refs[1]), (far_step(1 - lax.axis_index("tp")), pair_refs[3]))


def split_blocks(steps, gain_ref):
    blocks = []
    for step, pair_ref in steps:
        columns = pair_columns(step, 2 * pair_ref.shape[2])
        blocks.append((split_pair(pair_ref, gain_ref, columns), columns))
    return blocks


def normed_blocks(steps, gain_ref, inv_root):
    blocks = []
    for step, pair_ref in steps:
        columns = pair_columns(step, 2 * pair_ref.shape[2])
        blocks.append((normed_pair(pair_ref, gain_ref, columns, inv_root), columns))
    return blocks


def early_project_kernel(step, pair_ref, gain_ref, *refs):
    weight_refs, before_refs, total_ref = refs[:4], refs[4:-1], refs[-1]

    def finish(place, total):
        total = joined(total)
        for ref in before_refs:
            total = total + ref[:, place]
        total_ref[:, place] = total

    project_blocks(split_blocks(((step(), pair_ref),), gain_ref), weight_refs, finish)


def inverse_root(pair_refs):
    squares, width = 0.0, 0
    for pair_ref in pair_refs:
        rows = flat_pair(pair_ref)
        squares = squares + jnp.sum(rows * rows, axis=1, keepdims=True)
        width += rows.shape[1]
    return lax.rsqrt(squares / width + epsilon)


def project_kernel(chips, *refs):
    pair_refs, (early_ref, gain_ref) = refs[:chips], refs[chips : chips + 2]
    weight_refs = refs[chips + 2 : chips + 6]
    near_ref, mid_ref, far_ref, swap_ref, total_ref, made_ref = refs[chips + 6 :]
    core = lax.axis_index("tp")
    inv_root = inverse_root(pair_refs)

    def finish(place, total):
        total_ref[:, place] = early_ref[:, place] * inv_root + total

    project_blocks(normed_blocks(late_steps(pair_refs), gain_ref, inv_root), weight_refs, finish)
    heads, chan, _ = weight_refs[0].shape
    rows, lanes = total_ref.shape[0], 4 * chan
    product = total_ref[...]
    for head in range(heads):
        made_ref[pl.ds(head, rows, stride=heads), :] = product[:, head * lanes : (head + 1) * lanes]
    chip = lax.axis_index("kv")
    pairs = rows * heads // chips
    for step, sent_ref in placed_blocks(core, near_ref, mid_ref, far_ref, swap_ref):
        first = pl.multiple_of(lax.bitwise_xor(chip, step) * pairs, pairs)
        sent_ref[...] = made_ref[pl.ds(first, pairs), :].astype(jnp.bfloat16)


def sigmoid(x):
    small = jnp.exp(-jnp.abs(x))
    return jnp.where(x >= 0.0, 1.0, small) / (1.0 + small)


def readout_kernel(chips, *refs):
    got_refs, (bound_ref, state_ref, gain_ref) = refs[:chips], refs[chips : chips + 3]
    mixed_ref, key_ref, value_ref, placed_ref = refs[chips + 3 :]
    own_rows, heads, keys, _ = state_ref.shape
    chan = keys // chips
    chip, core = lax.axis_index("kv"), lax.axis_index("tp")
    for step, got_ref in placed_blocks(core, *got_refs):
        block = got_ref[...] if len(got_ref.shape) == 2 else got_ref[core]
        placed_ref[lax.bitwise_xor(chip, step)] = block.astype(jnp.float32)

    def channels(kind):
        return jnp.concatenate(
            [placed_ref[i][:, kind * chan : (kind + 1) * chan] for i in range(chips)], axis=1
        )

    pre_query, pre_forget, value_rows, pre_gate = (channels(kind) for kind in range(4))
    bound = jnp.concatenate([bound_ref[...]] * own_rows, axis=0)
    gain = jnp.concatenate([gain_ref[...]] * own_rows, axis=0)
    forget = bound + (1.0 - bound) * sigmoid(pre_forget)
    key_rows = (1.0 - bound) * sigmoid(-pre_forget)
    query = pre_query * sigmoid(pre_query)
    new_part = jnp.sum(query * key_rows, axis=1, keepdims=True) * value_rows
    weight = jnp.transpose(query * forget)
    old_parts = []
    for row in range(own_rows):
        for head in range(heads):
            pair = row * heads + head
            old_parts.append(
                jnp.sum(weight[:, pair : pair + 1] * state_ref[row, head], axis=0, keepdims=True)
            )
    readout = jnp.concatenate(old_parts, axis=0) + new_part
    inv_head = lax.rsqrt(jnp.mean(readout * readout, axis=1, keepdims=True) + epsilon)
    mixed = readout * inv_head * gain * (pre_gate * sigmoid(pre_gate))
    mixed_ref[...] = mixed.astype(jnp.bfloat16)
    key_ref[...] = key_rows
    value_ref[...] = value_rows


def state_kernel(key_ref, value_ref, state_ref, next_ref):
    own_rows, heads, _, _ = state_ref.shape
    key_cols = jnp.transpose(key_ref[...])
    for row in range(own_rows):
        for head in range(heads):
            pair = row * heads + head
            old = state_ref[row, head]
            next_ref[row, head] = old + key_cols[:, pair : pair + 1] * (
                value_ref[pair : pair + 1, :] - old
            )


def copy_out_kernel(made_ref, next_ref, done_ref):
    copy = pltpu.make_async_copy(made_ref, next_ref, done_ref)
    copy.start()
    copy.wait()


def stage_kernel(block_ref, staged_ref):
    staged_ref[...] = block_ref[...]


def out_kernel(chips, heads, *refs):
    pair_refs, (tokens_ref, weight_ref, residual_ref, placed_ref) = refs[:chips], refs[chips:]
    cores, pairs, values = pair_refs[0].shape
    own_rows = pairs // heads
    chip = lax.axis_index("kv")
    for step, pair_ref in placed_blocks(lax.axis_index("tp"), *pair_refs):
        first = pl.multiple_of(lax.bitwise_xor(chip, step) * (cores * pairs), cores * pairs)
        placed_ref[pl.ds(first, cores * pairs), :] = (
            pair_ref[...].astype(jnp.float32).reshape(-1, values)
        )
    blocks = []
    for core in range(cores):
        for head in range(heads):
            blocks.append(
                jnp.concatenate(
                    [
                        placed_ref[
                            pl.ds(core * pairs + row * heads + head, chips, stride=cores * pairs), :
                        ]
                        for row in range(own_rows)
                    ],
                    axis=0,
                )
            )
    mixed = jnp.concatenate(blocks, axis=1).astype(jnp.bfloat16)
    weight = weight_ref[...].reshape(-1, weight_ref.shape[2])
    projected = jnp.dot(mixed, weight, preferred_element_type=jnp.float32)
    ordered = [
        projected[row * chips + i : row * chips + i + 1]
        for i in range(chips)
        for row in range(own_rows)
    ]
    projected = jnp.concatenate(ordered, axis=0)
    residual_ref[...] = (tokens_ref[...].astype(jnp.float32) + projected).astype(jnp.bfloat16)


def down_part(hidden, down_ref, core, partial_ref):
    width = partial_ref.shape[2]
    chip = lax.axis_index("kv")
    far = lax.bitwise_xor(chip, far_step(core))
    columns = (2 * far, 2 * far + 1, 2 * lax.bitwise_xor(chip, 2) + core, 2 * chip + core)
    for slot, column in enumerate(columns):
        partial_ref[slot] = jnp.dot(
            hidden,
            down_ref[:, pl.ds(pl.multiple_of(column * width, width), width)],
            preferred_element_type=jnp.float32,
        )


def up_blocks(blocks, up_ref):
    total = None
    for rows, columns in blocks:
        part = jnp.dot(rows, up_ref[columns, :], preferred_element_type=jnp.float32)
        total = part if total is None else total + part
    return total


def early_up_kernel(step, pair_ref, gain_ref, up_ref, down_ref, *refs):
    del down_ref
    total = joined(up_blocks(split_blocks(((step(), pair_ref),), gain_ref), up_ref))
    for ref in refs[:-1]:
        total = total + ref[...]
    refs[-1][...] = total


def mixer_kernel(chips, *refs):
    pair_refs, (early_ref, gain_ref, up_ref, down_ref) = refs[:chips], refs[chips : chips + 4]
    hidden_ref, partial_ref = refs[chips + 4 :]
    inv_root = inverse_root(pair_refs)
    late = up_blocks(normed_blocks(late_steps(pair_refs), gain_ref, inv_root), up_ref)
    hidden = early_ref[...] * inv_root + late
    hidden = jnp.square(jnp.maximum(hidden, 0.0)).astype(jnp.bfloat16)
    hidden_ref[...] = hidden
    down_part(hidden, down_ref, 1 - lax.axis_index("tp"), partial_ref)


def own_part_kernel(hidden_ref, down_ref, partial_ref):
    down_part(hidden_ref[...], down_ref, lax.axis_index("tp"), partial_ref)


def chip_sum_kernel(own_ref, mate_ref, far_ref, mid_ref, kept_ref):
    for core in range(2):
        far_ref[core] = (own_ref[core] + mate_ref[core]).astype(jnp.bfloat16)
    mid_ref[...] = (own_ref[2] + mate_ref[2]).astype(jnp.bfloat16)
    kept_ref[...] = own_ref[3] + mate_ref[3]


def last_kernel(residual_ref, kept_ref, mid_ref, far_ref, swapped_ref, output_ref):
    core = lax.axis_index("tp")
    total = kept_ref[...]
    for block in (mid_ref[...], far_ref[core], swapped_ref[core]):
        total = total + block.astype(jnp.float32)
    output_ref[...] = (residual_ref[...].astype(jnp.float32) + total).astype(jnp.bfloat16)


MIB = 1 << 20
COST = (10**11, 10**11, 10**9, 10**9, 10**6, 10**6, 10**9, 10**6, 10**6, 10**9, 10**6)


def tiled_local(
    kv,
    tp,
    tokens,
    mix_gain,
    query_weight,
    forget_weight,
    value_weight,
    gate_weight,
    lower_bound,
    recurrent_state,
    head_gain,
    out_weight,
    mlp_gain,
    up_weight,
    down_weight,
):
    rows, width = tokens.shape
    heads, chan, _ = query_weight.shape
    own_rows, _, keys, values = recurrent_state.shape
    pairs = own_rows * heads
    shape = jax.ShapeDtypeStruct
    f32, bf16 = jnp.float32, jnp.bfloat16

    def permute(block, steps, swapped=False):
        hops = [
            (k * tp + t, (k ^ steps[t]) * tp + (1 - t if swapped else t))
            for k in range(kv)
            for t in range(tp)
        ]
        return lax.ppermute(block, group, hops)

    def other_core(block):
        return permute(block, (0, 0), True)

    def paired(block, mate, cost):
        return call(pair_kernel, shape((tp,) + block.shape, block.dtype), (block, mate), cost, MIB)

    def crossed(far, mid):
        got_far = permute(far, (1, 3))
        got_mid = permute(mid, (2, 2))
        return got_mid, got_far, permute(got_far, (0, 0), True)

    def gather_pairs(block, staged, cost):
        pair = paired(staged, other_core(block), cost)
        return (pair,) + crossed(pair, pair)

    def early_parts(kernel, got, operands, columns, cost):
        total = ()
        for place, step in ((0, near_step), (2, other_step)):
            part = call(
                functools.partial(kernel, step),
                shape((rows, columns), f32),
                (got[place], *operands, *total),
                cost,
                14 * MIB,
            )
            total = (part,)
        return total[0]

    staged = call(stage_kernel, shape(tokens.shape, bf16), (tokens,), COST[4], MIB)
    pairs_of_rows = gather_pairs(tokens, staged, COST[0])
    mix_row = mix_gain.reshape(1, -1)
    projections = (query_weight, forget_weight, value_weight, gate_weight)
    early = early_parts(
        early_project_kernel, pairs_of_rows, (mix_row, *projections), 4 * heads * chan, COST[9]
    )
    near, mid, far, swap = call(
        functools.partial(project_kernel, kv),
        [shape((pairs, 4 * chan), bf16)] * kv,
        (*pairs_of_rows, early, mix_row, *projections),
        COST[1],
        14 * MIB,
        [pltpu.VMEM((rows, 4 * heads * chan), f32), pltpu.VMEM((rows * heads, 4 * chan), f32)],
    )
    got = (near,) + crossed(paired(far, other_core(swap), COST[4]), mid)
    mixed, key_rows, value_rows = call(
        functools.partial(readout_kernel, kv),
        [shape((pairs, values), bf16), shape((pairs, keys), f32), shape((pairs, values), f32)],
        (*got, lower_bound, recurrent_state, head_gain),
        COST[2],
        14 * MIB,
        [pltpu.VMEM((kv, pairs, 4 * chan), f32)],
    )
    next_state = call(
        state_kernel,
        pltpu.VMEM(recurrent_state.shape, f32),
        (key_rows, value_rows, recurrent_state),
        COST[3],
        4 * MIB,
    )
    next_state = pl.pallas_call(
        copy_out_kernel,
        out_shape=shape(recurrent_state.shape, f32),
        in_specs=[whole],
        out_specs=pl.BlockSpec(memory_space=pl.ANY),
        scratch_shapes=[pltpu.SemaphoreType.DMA],
        compiler_params=pltpu.CompilerParams(vmem_limit_bytes=MIB),
        cost_estimate=pl.CostEstimate(flops=COST[3], bytes_accessed=0, transcendentals=0),
    )(next_state)
    residual = call(
        functools.partial(out_kernel, kv, heads),
        shape((rows, width), bf16),
        (*gather_pairs(mixed, mixed, COST[4]), tokens, out_weight),
        COST[4],
        14 * MIB,
        [pltpu.VMEM((kv * tp * pairs, values), f32)],
    )
    pairs_of_rows = gather_pairs(residual, residual, COST[4])
    mlp_row = mlp_gain.reshape(1, -1)
    early = early_parts(
        early_up_kernel, pairs_of_rows, (mlp_row, up_weight, down_weight), up_weight.shape[1], COST[10]
    )
    hidden, mate_part = call(
        functools.partial(mixer_kernel, kv),
        [shape((rows, up_weight.shape[1]), bf16), shape((kv, rows, width), f32)],
        (*pairs_of_rows, early, mlp_row, up_weight, down_weight),
        COST[5],
        14 * MIB,
    )
    own_part = call(
        own_part_kernel, shape((kv, rows, width), f32), (hidden, down_weight), COST[6], 14 * MIB
    )
    far, mid, kept = call(
        chip_sum_kernel,
        [shape((tp, rows, width), bf16), shape((rows, width), bf16), shape((rows, width), f32)],
        (own_part, other_core(mate_part)),
        COST[7],
        MIB,
    )
    sums = crossed(far, mid)
    layer_output = call(
        last_kernel, shape((rows, width), bf16), (residual, kept, *sums), COST[8], MIB
    )
    return (layer_output, next_state)


def tiles(kv, tp, tokens, query_weight):
    rows, width = tokens.shape
    aligned = rows % 8 == 0 and width % 128 == 0 and query_weight.shape[1] % 32 == 0
    return aligned and tp == 2 and kv == 4


def solution(mesh):
    placed = (
        P("dp", ("kv", "tp")),
        P(),
        P("tp", "kv", None),
        P("tp", "kv", None),
        P("tp", "kv", None),
        P("tp", "kv", None),
        P("tp", None),
        P(("dp", "kv"), "tp", None, None),
        P("tp", None),
        P(None, None, ("kv", "tp")),
        P(),
        P(None, ("kv", "tp")),
        P(("kv", "tp"), None),
    )

    def body(*arrays):
        kv, tp = mesh.shape["kv"], mesh.shape["tp"]
        run = tiled_local if tiles(kv, tp, arrays[0], arrays[2]) else local
        return run(kv, tp, *arrays)

    return jax.shard_map(
        body,
        mesh=mesh,
        in_specs=placed,
        out_specs=(P("dp", ("kv", "tp")), P(("dp", "kv"), "tp", None, None)),
        check_vma=False,
    )
```

```python
import functools

import jax
import jax.numpy as jnp
from jax import lax
from jax.experimental import pallas as pl
from jax.experimental.pallas import tpu as pltpu
from jax.sharding import PartitionSpec as P


epsilon = 1e-06
group = ("kv", "tp")


def gather_blocks(block, members):
    copies = lax.optimization_barrier(jnp.broadcast_to(block[None], (members,) + block.shape))
    return lax.all_to_all(copies, group, split_axis=0, concat_axis=0, tiled=True)


def whole_rows(row_block, members):
    pieces = gather_blocks(row_block, members)
    return jnp.swapaxes(pieces, 0, 1).reshape(row_block.shape[0], -1)


def normed_rows(rows, gain_vector):
    rows = rows.astype(jnp.float32)
    inv_root = lax.rsqrt(jnp.mean(rows * rows, axis=1, keepdims=True) + epsilon)
    return (rows * inv_root * gain_vector).astype(jnp.bfloat16)


def local(
    kv,
    tp,
    tokens,
    mix_gain,
    query_weight,
    forget_weight,
    value_weight,
    gate_weight,
    lower_bound,
    recurrent_state,
    head_gain,
    out_weight,
    mlp_gain,
    up_weight,
    down_weight,
):
    members = kv * tp
    normed = normed_rows(whole_rows(tokens, members), mix_gain)
    local_heads, local_chan, width = query_weight.shape
    rows = normed.shape[0]
    own_rows = rows // kv
    products = [
        lax.dot_general(
            normed,
            weight.reshape(-1, width),
            (((1,), (1,)), ((), ())),
            preferred_element_type=jnp.float32,
        ).astype(jnp.bfloat16)
        for weight in (query_weight, forget_weight, value_weight, gate_weight)
    ]
    product = jnp.stack(products, axis=1).reshape(kv, own_rows * 4 * local_heads, local_chan)
    exchanged = lax.all_to_all(product, "kv", split_axis=0, concat_axis=0, tiled=True)
    channels = jnp.moveaxis(exchanged.reshape(kv, own_rows, 4, local_heads, local_chan), 0, 3)
    channels = channels.reshape(own_rows, 4, local_heads, kv * local_chan).astype(jnp.float32)
    pre_query, pre_forget, value_rows, pre_gate = (channels[:, i] for i in range(4))
    log_forget = jnp.logaddexp(
        jnp.log(lower_bound),
        jnp.log1p(-lower_bound) + jax.nn.log_sigmoid(pre_forget),
    )
    key_rows = -jnp.expm1(log_forget)
    next_state = (
        jnp.exp(log_forget)[:, :, :, None] * recurrent_state
        + key_rows[:, :, :, None] * value_rows[:, :, None, :]
    )
    query_act = jax.nn.silu(pre_query)
    readout = jnp.einsum("bhk,bhkv->bhv", query_act, next_state, precision=lax.Precision.HIGHEST)
    inv_head = lax.rsqrt(jnp.mean(readout * readout, axis=2, keepdims=True) + epsilon)
    mixed_heads = (readout * inv_head * head_gain * jax.nn.silu(pre_gate)).astype(jnp.bfloat16)
    mixed = gather_blocks(mixed_heads.reshape(own_rows, -1), members)
    mixed = jnp.swapaxes(mixed.reshape(kv, tp, own_rows, -1), 1, 2).reshape(rows, -1)
    out_matrix = out_weight.reshape(-1, out_weight.shape[2])
    projected = jnp.dot(mixed, out_matrix, preferred_element_type=jnp.float32)
    residual = lax.optimization_barrier(
        (tokens.astype(jnp.float32) + projected).astype(jnp.bfloat16)
    )
    normed_mlp = normed_rows(whole_rows(residual, members), mlp_gain)
    hidden = jnp.square(
        jax.nn.relu(jnp.dot(normed_mlp, up_weight, preferred_element_type=jnp.float32))
    ).astype(jnp.bfloat16)
    partial = jnp.dot(hidden, down_weight, preferred_element_type=jnp.float32)
    partial = jnp.swapaxes(partial.reshape(rows, members, -1), 0, 1)
    summed = lax.all_to_all(partial, group, split_axis=0, concat_axis=0, tiled=True).sum(axis=0)
    layer_output = (residual.astype(jnp.float32) + summed).astype(jnp.bfloat16)
    return (layer_output, next_state)


whole = pl.BlockSpec(memory_space=pltpu.VMEM)


def call(body, outs, arrays, flops, limit, scratch=()):
    return pl.pallas_call(
        body,
        out_shape=outs,
        in_specs=[whole] * len(arrays),
        out_specs=jax.tree.map(lambda _: whole, outs),
        scratch_shapes=scratch,
        compiler_params=pltpu.CompilerParams(vmem_limit_bytes=limit),
        cost_estimate=pl.CostEstimate(flops=flops, bytes_accessed=0, transcendentals=0),
    )(*arrays)


def far_step(core):
    return 1 + core


def placed_blocks(core, near_ref, mid_ref, far_ref, swapped_ref):
    return (
        (0, near_ref),
        (3, mid_ref),
        (far_step(core), far_ref),
        (far_step(1 - core), swapped_ref),
    )


def pair_kernel(own_ref, mate_ref, pair_ref):
    core = lax.axis_index("tp")
    pair_ref[core] = own_ref[...]
    pair_ref[1 - core] = mate_ref[...]


def pair_columns(step, width):
    first = lax.bitwise_xor(lax.axis_index("kv"), step) * width
    return pl.ds(pl.multiple_of(first, width), width)


def flat_pair(pair_ref):
    return jnp.concatenate([pair_ref[0], pair_ref[1]], axis=1).astype(jnp.float32)


def split_pair(pair_ref, gain_ref, columns):
    scaled = flat_pair(pair_ref) * gain_ref[:, columns]
    high = scaled.astype(jnp.bfloat16)
    low = (scaled - high.astype(jnp.float32)).astype(jnp.bfloat16)
    return jnp.concatenate([high, low], axis=0)


def normed_pair(pair_ref, gain_ref, columns, inv_root):
    return (flat_pair(pair_ref) * inv_root * gain_ref[:, columns]).astype(jnp.bfloat16)


def joined(product):
    half = product.shape[0] // 2
    return product[:half] + product[half:]


def head_weight(weight_refs, head, columns):
    return jnp.concatenate(
        [ref[one, :, columns] for one in (head, head + 1) for ref in weight_refs], axis=0
    )


def project_blocks(blocks, weight_refs, finish):
    heads, chan, _ = weight_refs[0].shape
    lanes = 8 * chan
    for head in range(0, heads, 2):
        total = None
        for rows, columns in blocks:
            part = lax.dot_general(
                rows,
                head_weight(weight_refs, head, columns),
                (((1,), (1,)), ((), ())),
                preferred_element_type=jnp.float32,
            )
            total = part if total is None else total + part
        finish(slice(head // 2 * lanes, (head // 2 + 1) * lanes), total)


def near_step():
    return 0


def other_step():
    return far_step(lax.axis_index("tp"))


def swapped_step():
    return far_step(1 - lax.axis_index("tp"))


def late_steps(pair_refs):
    return ((3, pair_refs[1]),)


def split_blocks(steps, gain_ref):
    blocks = []
    for step, pair_ref in steps:
        columns = pair_columns(step, 2 * pair_ref.shape[2])
        blocks.append((split_pair(pair_ref, gain_ref, columns), columns))
    return blocks


def normed_blocks(steps, gain_ref, inv_root):
    blocks = []
    for step, pair_ref in steps:
        columns = pair_columns(step, 2 * pair_ref.shape[2])
        blocks.append((normed_pair(pair_ref, gain_ref, columns, inv_root), columns))
    return blocks


def early_project_kernel(step, pair_ref, gain_ref, *refs):
    weight_refs, before_refs, total_ref = refs[:4], refs[4:-1], refs[-1]

    def finish(place, total):
        total = joined(total)
        for ref in before_refs:
            total = total + ref[:, place]
        total_ref[:, place] = total

    project_blocks(split_blocks(((step(), pair_ref),), gain_ref), weight_refs, finish)


def inverse_root(pair_refs):
    squares, width = 0.0, 0
    for pair_ref in pair_refs:
        rows = flat_pair(pair_ref)
        squares = squares + jnp.sum(rows * rows, axis=1, keepdims=True)
        width += rows.shape[1]
    return lax.rsqrt(squares / width + epsilon)


def project_kernel(chips, *refs):
    pair_refs, (early_ref, gain_ref) = refs[:chips], refs[chips : chips + 2]
    weight_refs = refs[chips + 2 : chips + 6]
    near_ref, mid_ref, far_ref, swap_ref, total_ref, made_ref = refs[chips + 6 :]
    core = lax.axis_index("tp")
    inv_root = inverse_root(pair_refs)

    def finish(place, total):
        total_ref[:, place] = early_ref[:, place] * inv_root + total

    project_blocks(normed_blocks(late_steps(pair_refs), gain_ref, inv_root), weight_refs, finish)
    heads, chan, _ = weight_refs[0].shape
    rows, lanes = total_ref.shape[0], 4 * chan
    product = total_ref[...]
    for head in range(heads):
        made_ref[pl.ds(head, rows, stride=heads), :] = product[:, head * lanes : (head + 1) * lanes]
    chip = lax.axis_index("kv")
    pairs = rows * heads // chips
    for step, sent_ref in placed_blocks(core, near_ref, mid_ref, far_ref, swap_ref):
        first = pl.multiple_of(lax.bitwise_xor(chip, step) * pairs, pairs)
        sent_ref[...] = made_ref[pl.ds(first, pairs), :].astype(jnp.bfloat16)


def sigmoid(x):
    small = jnp.exp(-jnp.abs(x))
    return jnp.where(x >= 0.0, 1.0, small) / (1.0 + small)


def readout_kernel(chips, *refs):
    got_refs, (bound_ref, state_ref, gain_ref) = refs[:chips], refs[chips : chips + 3]
    mixed_ref, key_ref, value_ref, placed_ref = refs[chips + 3 :]
    own_rows, heads, keys, _ = state_ref.shape
    chan = keys // chips
    chip, core = lax.axis_index("kv"), lax.axis_index("tp")
    for step, got_ref in placed_blocks(core, *got_refs):
        block = got_ref[...] if len(got_ref.shape) == 2 else got_ref[core]
        placed_ref[lax.bitwise_xor(chip, step)] = block.astype(jnp.float32)

    def channels(kind):
        return jnp.concatenate(
            [placed_ref[i][:, kind * chan : (kind + 1) * chan] for i in range(chips)], axis=1
        )

    pre_query, pre_forget, value_rows, pre_gate = (channels(kind) for kind in range(4))
    bound = jnp.concatenate([bound_ref[...]] * own_rows, axis=0)
    gain = jnp.concatenate([gain_ref[...]] * own_rows, axis=0)
    forget = bound + (1.0 - bound) * sigmoid(pre_forget)
    key_rows = (1.0 - bound) * sigmoid(-pre_forget)
    query = pre_query * sigmoid(pre_query)
    new_part = jnp.sum(query * key_rows, axis=1, keepdims=True) * value_rows
    weight = jnp.transpose(query * forget)
    old_parts = []
    for row in range(own_rows):
        for head in range(heads):
            pair = row * heads + head
            old_parts.append(
                jnp.sum(weight[:, pair : pair + 1] * state_ref[row, head], axis=0, keepdims=True)
            )
    readout = jnp.concatenate(old_parts, axis=0) + new_part
    inv_head = lax.rsqrt(jnp.mean(readout * readout, axis=1, keepdims=True) + epsilon)
    mixed = readout * inv_head * gain * (pre_gate * sigmoid(pre_gate))
    mixed_ref[...] = mixed.astype(jnp.bfloat16)
    key_ref[...] = key_rows
    value_ref[...] = value_rows


def state_kernel(key_ref, value_ref, state_ref, next_ref):
    own_rows, heads, _, _ = state_ref.shape
    key_cols = jnp.transpose(key_ref[...])
    for row in range(own_rows):
        for head in range(heads):
            pair = row * heads + head
            old = state_ref[row, head]
            next_ref[row, head] = old + key_cols[:, pair : pair + 1] * (
                value_ref[pair : pair + 1, :] - old
            )


def copy_out_kernel(made_ref, next_ref, done_ref):
    copy = pltpu.make_async_copy(made_ref, next_ref, done_ref)
    copy.start()
    copy.wait()


def stage_kernel(block_ref, staged_ref):
    staged_ref[...] = block_ref[...]


def out_kernel(chips, heads, *refs):
    pair_refs, (tokens_ref, weight_ref, residual_ref, placed_ref) = refs[:chips], refs[chips:]
    cores, pairs, values = pair_refs[0].shape
    own_rows = pairs // heads
    chip = lax.axis_index("kv")
    for step, pair_ref in placed_blocks(lax.axis_index("tp"), *pair_refs):
        first = pl.multiple_of(lax.bitwise_xor(chip, step) * (cores * pairs), cores * pairs)
        placed_ref[pl.ds(first, cores * pairs), :] = (
            pair_ref[...].astype(jnp.float32).reshape(-1, values)
        )
    blocks = []
    for core in range(cores):
        for head in range(heads):
            blocks.append(
                jnp.concatenate(
                    [
                        placed_ref[
                            pl.ds(core * pairs + row * heads + head, chips, stride=cores * pairs), :
                        ]
                        for row in range(own_rows)
                    ],
                    axis=0,
                )
            )
    mixed = jnp.concatenate(blocks, axis=1).astype(jnp.bfloat16)
    weight = weight_ref[...].reshape(-1, weight_ref.shape[2])
    projected = jnp.dot(mixed, weight, preferred_element_type=jnp.float32)
    ordered = [
        projected[row * chips + i : row * chips + i + 1]
        for i in range(chips)
        for row in range(own_rows)
    ]
    projected = jnp.concatenate(ordered, axis=0)
    residual_ref[...] = (tokens_ref[...].astype(jnp.float32) + projected).astype(jnp.bfloat16)


def down_part(hidden, down_ref, core, partial_ref):
    width = partial_ref.shape[2]
    chip = lax.axis_index("kv")
    far = lax.bitwise_xor(chip, far_step(core))
    columns = (2 * far, 2 * far + 1, 2 * lax.bitwise_xor(chip, 3) + core, 2 * chip + core)
    for slot, column in enumerate(columns):
        partial_ref[slot] = jnp.dot(
            hidden,
            down_ref[:, pl.ds(pl.multiple_of(column * width, width), width)],
            preferred_element_type=jnp.float32,
        )


def up_blocks(blocks, up_ref):
    total = None
    for rows, columns in blocks:
        part = jnp.dot(rows, up_ref[columns, :], preferred_element_type=jnp.float32)
        total = part if total is None else total + part
    return total


def early_up_kernel(step, pair_ref, gain_ref, up_ref, down_ref, *refs):
    del down_ref
    total = joined(up_blocks(split_blocks(((step(), pair_ref),), gain_ref), up_ref))
    for ref in refs[:-1]:
        total = total + ref[...]
    refs[-1][...] = total


def mixer_kernel(chips, *refs):
    pair_refs, (early_ref, gain_ref, up_ref, down_ref) = refs[:chips], refs[chips : chips + 4]
    hidden_ref, partial_ref = refs[chips + 4 :]
    inv_root = inverse_root(pair_refs)
    late = up_blocks(normed_blocks(late_steps(pair_refs), gain_ref, inv_root), up_ref)
    hidden = early_ref[...] * inv_root + late
    hidden = jnp.square(jnp.maximum(hidden, 0.0)).astype(jnp.bfloat16)
    hidden_ref[...] = hidden
    down_part(hidden, down_ref, 1 - lax.axis_index("tp"), partial_ref)


def own_part_kernel(hidden_ref, down_ref, partial_ref):
    down_part(hidden_ref[...], down_ref, lax.axis_index("tp"), partial_ref)


def chip_sum_kernel(own_ref, mate_ref, far_ref, mid_ref, kept_ref):
    for core in range(2):
        far_ref[core] = (own_ref[core] + mate_ref[core]).astype(jnp.bfloat16)
    mid_ref[...] = (own_ref[2] + mate_ref[2]).astype(jnp.bfloat16)
    kept_ref[...] = own_ref[3] + mate_ref[3]


def last_kernel(residual_ref, kept_ref, mid_ref, far_ref, swapped_ref, output_ref):
    core = lax.axis_index("tp")
    total = kept_ref[...]
    for block in (mid_ref[...], far_ref[core], swapped_ref[core]):
        total = total + block.astype(jnp.float32)
    output_ref[...] = (residual_ref[...].astype(jnp.float32) + total).astype(jnp.bfloat16)


MIB = 1 << 20
COST = (10**11, 10**11, 10**9, 10**9, 10**6, 10**6, 10**9, 10**6, 10**6, 10**9, 10**6)


def tiled_local(
    kv,
    tp,
    tokens,
    mix_gain,
    query_weight,
    forget_weight,
    value_weight,
    gate_weight,
    lower_bound,
    recurrent_state,
    head_gain,
    out_weight,
    mlp_gain,
    up_weight,
    down_weight,
):
    rows, width = tokens.shape
    heads, chan, _ = query_weight.shape
    own_rows, _, keys, values = recurrent_state.shape
    pairs = own_rows * heads
    shape = jax.ShapeDtypeStruct
    f32, bf16 = jnp.float32, jnp.bfloat16

    def permute(block, steps, swapped=False):
        hops = [
            (k * tp + t, (k ^ steps[t]) * tp + (1 - t if swapped else t))
            for k in range(kv)
            for t in range(tp)
        ]
        return lax.ppermute(block, group, hops)

    def other_core(block):
        return permute(block, (0, 0), True)

    def paired(block, mate, cost):
        return call(pair_kernel, shape((tp,) + block.shape, block.dtype), (block, mate), cost, MIB)

    def crossed(far, mid):
        got_far = permute(far, (1, 2))
        got_mid = permute(mid, (3, 3))
        return got_mid, got_far, permute(got_far, (0, 0), True)

    def gather_pairs(block, staged, cost):
        pair = paired(staged, other_core(block), cost)
        return (pair,) + crossed(pair, pair)

    def early_parts(kernel, got, operands, columns, cost):
        total = ()
        for place, step in ((0, near_step), (2, other_step), (3, swapped_step)):
            part = call(
                functools.partial(kernel, step),
                shape((rows, columns), f32),
                (got[place], *operands, *total),
                cost,
                14 * MIB,
            )
            total = (part,)
        return total[0]

    staged = call(stage_kernel, shape(tokens.shape, bf16), (tokens,), COST[4], MIB)
    pairs_of_rows = gather_pairs(tokens, staged, COST[0])
    mix_row = mix_gain.reshape(1, -1)
    projections = (query_weight, forget_weight, value_weight, gate_weight)
    early = early_parts(
        early_project_kernel, pairs_of_rows, (mix_row, *projections), 4 * heads * chan, COST[9]
    )
    near, mid, far, swap = call(
        functools.partial(project_kernel, kv),
        [shape((pairs, 4 * chan), bf16)] * kv,
        (*pairs_of_rows, early, mix_row, *projections),
        COST[1],
        14 * MIB,
        [pltpu.VMEM((rows, 4 * heads * chan), f32), pltpu.VMEM((rows * heads, 4 * chan), f32)],
    )
    got = (near,) + crossed(paired(far, other_core(swap), COST[4]), mid)
    mixed, key_rows, value_rows = call(
        functools.partial(readout_kernel, kv),
        [shape((pairs, values), bf16), shape((pairs, keys), f32), shape((pairs, values), f32)],
        (*got, lower_bound, recurrent_state, head_gain),
        COST[2],
        14 * MIB,
        [pltpu.VMEM((kv, pairs, 4 * chan), f32)],
    )
    next_state = call(
        state_kernel,
        pltpu.VMEM(recurrent_state.shape, f32),
        (key_rows, value_rows, recurrent_state),
        COST[3],
        4 * MIB,
    )
    next_state = pl.pallas_call(
        copy_out_kernel,
        out_shape=shape(recurrent_state.shape, f32),
        in_specs=[whole],
        out_specs=pl.BlockSpec(memory_space=pl.ANY),
        scratch_shapes=[pltpu.SemaphoreType.DMA],
        compiler_params=pltpu.CompilerParams(vmem_limit_bytes=MIB),
        cost_estimate=pl.CostEstimate(flops=COST[3], bytes_accessed=0, transcendentals=0),
    )(next_state)
    residual = call(
        functools.partial(out_kernel, kv, heads),
        shape((rows, width), bf16),
        (*gather_pairs(mixed, mixed, COST[4]), tokens, out_weight),
        COST[4],
        14 * MIB,
        [pltpu.VMEM((kv * tp * pairs, values), f32)],
    )
    pairs_of_rows = gather_pairs(residual, residual, COST[4])
    mlp_row = mlp_gain.reshape(1, -1)
    early = early_parts(
        early_up_kernel, pairs_of_rows, (mlp_row, up_weight, down_weight), up_weight.shape[1], COST[10]
    )
    hidden, mate_part = call(
        functools.partial(mixer_kernel, kv),
        [shape((rows, up_weight.shape[1]), bf16), shape((kv, rows, width), f32)],
        (*pairs_of_rows, early, mlp_row, up_weight, down_weight),
        COST[5],
        14 * MIB,
    )
    own_part = call(
        own_part_kernel, shape((kv, rows, width), f32), (hidden, down_weight), COST[6], 14 * MIB
    )
    far, mid, kept = call(
        chip_sum_kernel,
        [shape((tp, rows, width), bf16), shape((rows, width), bf16), shape((rows, width), f32)],
        (own_part, other_core(mate_part)),
        COST[7],
        MIB,
    )
    sums = crossed(far, mid)
    layer_output = call(
        last_kernel, shape((rows, width), bf16), (residual, kept, *sums), COST[8], MIB
    )
    return (layer_output, next_state)


def tiles(kv, tp, tokens, query_weight):
    rows, width = tokens.shape
    aligned = rows % 8 == 0 and width % 128 == 0 and query_weight.shape[1] % 32 == 0
    return aligned and tp == 2 and kv == 4


def solution(mesh):
    placed = (
        P("dp", ("kv", "tp")),
        P(),
        P("tp", "kv", None),
        P("tp", "kv", None),
        P("tp", "kv", None),
        P("tp", "kv", None),
        P("tp", None),
        P(("dp", "kv"), "tp", None, None),
        P("tp", None),
        P(None, None, ("kv", "tp")),
        P(),
        P(None, ("kv", "tp")),
        P(("kv", "tp"), None),
    )

    def body(*arrays):
        kv, tp = mesh.shape["kv"], mesh.shape["tp"]
        run = tiled_local if tiles(kv, tp, arrays[0], arrays[2]) else local
        return run(kv, tp, *arrays)

    return jax.shard_map(
        body,
        mesh=mesh,
        in_specs=placed,
        out_specs=(P("dp", ("kv", "tp")), P(("dp", "kv"), "tp", None, None)),
        check_vma=False,
    )
```

```python
import functools

import jax
import jax.numpy as jnp
from jax import lax
from jax.experimental import pallas as pl
from jax.experimental.pallas import tpu as pltpu
from jax.sharding import PartitionSpec as P


epsilon = 1e-06
group = ("kv", "tp")


def gather_blocks(block, members):
    copies = lax.optimization_barrier(jnp.broadcast_to(block[None], (members,) + block.shape))
    return lax.all_to_all(copies, group, split_axis=0, concat_axis=0, tiled=True)


def whole_rows(row_block, members):
    pieces = gather_blocks(row_block, members)
    return jnp.swapaxes(pieces, 0, 1).reshape(row_block.shape[0], -1)


def normed_rows(rows, gain_vector):
    rows = rows.astype(jnp.float32)
    inv_root = lax.rsqrt(jnp.mean(rows * rows, axis=1, keepdims=True) + epsilon)
    return (rows * inv_root * gain_vector).astype(jnp.bfloat16)


def local(
    kv,
    tp,
    tokens,
    mix_gain,
    query_weight,
    forget_weight,
    value_weight,
    gate_weight,
    lower_bound,
    recurrent_state,
    head_gain,
    out_weight,
    mlp_gain,
    up_weight,
    down_weight,
):
    members = kv * tp
    normed = normed_rows(whole_rows(tokens, members), mix_gain)
    local_heads, local_chan, width = query_weight.shape
    rows = normed.shape[0]
    own_rows = rows // kv
    products = [
        lax.dot_general(
            normed,
            weight.reshape(-1, width),
            (((1,), (1,)), ((), ())),
            preferred_element_type=jnp.float32,
        ).astype(jnp.bfloat16)
        for weight in (query_weight, forget_weight, value_weight, gate_weight)
    ]
    product = jnp.stack(products, axis=1).reshape(kv, own_rows * 4 * local_heads, local_chan)
    exchanged = lax.all_to_all(product, "kv", split_axis=0, concat_axis=0, tiled=True)
    channels = jnp.moveaxis(exchanged.reshape(kv, own_rows, 4, local_heads, local_chan), 0, 3)
    channels = channels.reshape(own_rows, 4, local_heads, kv * local_chan).astype(jnp.float32)
    pre_query, pre_forget, value_rows, pre_gate = (channels[:, i] for i in range(4))
    log_forget = jnp.logaddexp(
        jnp.log(lower_bound),
        jnp.log1p(-lower_bound) + jax.nn.log_sigmoid(pre_forget),
    )
    key_rows = -jnp.expm1(log_forget)
    next_state = (
        jnp.exp(log_forget)[:, :, :, None] * recurrent_state
        + key_rows[:, :, :, None] * value_rows[:, :, None, :]
    )
    query_act = jax.nn.silu(pre_query)
    readout = jnp.einsum("bhk,bhkv->bhv", query_act, next_state, precision=lax.Precision.HIGHEST)
    inv_head = lax.rsqrt(jnp.mean(readout * readout, axis=2, keepdims=True) + epsilon)
    mixed_heads = (readout * inv_head * head_gain * jax.nn.silu(pre_gate)).astype(jnp.bfloat16)
    mixed = gather_blocks(mixed_heads.reshape(own_rows, -1), members)
    mixed = jnp.swapaxes(mixed.reshape(kv, tp, own_rows, -1), 1, 2).reshape(rows, -1)
    out_matrix = out_weight.reshape(-1, out_weight.shape[2])
    projected = jnp.dot(mixed, out_matrix, preferred_element_type=jnp.float32)
    residual = lax.optimization_barrier(
        (tokens.astype(jnp.float32) + projected).astype(jnp.bfloat16)
    )
    normed_mlp = normed_rows(whole_rows(residual, members), mlp_gain)
    hidden = jnp.square(
        jax.nn.relu(jnp.dot(normed_mlp, up_weight, preferred_element_type=jnp.float32))
    ).astype(jnp.bfloat16)
    partial = jnp.dot(hidden, down_weight, preferred_element_type=jnp.float32)
    partial = jnp.swapaxes(partial.reshape(rows, members, -1), 0, 1)
    summed = lax.all_to_all(partial, group, split_axis=0, concat_axis=0, tiled=True).sum(axis=0)
    layer_output = (residual.astype(jnp.float32) + summed).astype(jnp.bfloat16)
    return (layer_output, next_state)


whole = pl.BlockSpec(memory_space=pltpu.VMEM)


def call(body, outs, arrays, flops, limit, scratch=()):
    return pl.pallas_call(
        body,
        out_shape=outs,
        in_specs=[whole] * len(arrays),
        out_specs=jax.tree.map(lambda _: whole, outs),
        scratch_shapes=scratch,
        compiler_params=pltpu.CompilerParams(vmem_limit_bytes=limit),
        cost_estimate=pl.CostEstimate(flops=flops, bytes_accessed=0, transcendentals=0),
    )(*arrays)


def far_step(core):
    return 1 + core


def placed_blocks(core, near_ref, mid_ref, far_ref, swapped_ref):
    return (
        (0, near_ref),
        (3, mid_ref),
        (far_step(core), far_ref),
        (far_step(1 - core), swapped_ref),
    )


def pair_kernel(own_ref, mate_ref, pair_ref):
    core = lax.axis_index("tp")
    pair_ref[core] = own_ref[...]
    pair_ref[1 - core] = mate_ref[...]


def pair_columns(step, width):
    first = lax.bitwise_xor(lax.axis_index("kv"), step) * width
    return pl.ds(pl.multiple_of(first, width), width)


def flat_pair(pair_ref):
    return jnp.concatenate([pair_ref[0], pair_ref[1]], axis=1).astype(jnp.float32)


def split_pair(pair_ref, gain_ref, columns):
    scaled = flat_pair(pair_ref) * gain_ref[:, columns]
    high = scaled.astype(jnp.bfloat16)
    low = (scaled - high.astype(jnp.float32)).astype(jnp.bfloat16)
    return jnp.concatenate([high, low], axis=0)


def normed_pair(pair_ref, gain_ref, columns, inv_root):
    return (flat_pair(pair_ref) * inv_root * gain_ref[:, columns]).astype(jnp.bfloat16)


def joined(product):
    half = product.shape[0] // 2
    return product[:half] + product[half:]


def head_weight(weight_refs, head, columns):
    return jnp.concatenate(
        [ref[one, :, columns] for one in (head, head + 1) for ref in weight_refs], axis=0
    )


def project_blocks(blocks, weight_refs, finish):
    heads, chan, _ = weight_refs[0].shape
    lanes = 8 * chan
    for head in range(0, heads, 2):
        total = None
        for rows, columns in blocks:
            part = lax.dot_general(
                rows,
                head_weight(weight_refs, head, columns),
                (((1,), (1,)), ((), ())),
                preferred_element_type=jnp.float32,
            )
            total = part if total is None else total + part
        finish(slice(head // 2 * lanes, (head // 2 + 1) * lanes), total)


def near_step():
    return 0


def other_step():
    return far_step(lax.axis_index("tp"))


def swapped_step():
    return far_step(1 - lax.axis_index("tp"))


def late_steps(pair_refs):
    return ((3, pair_refs[1]),)


def split_blocks(steps, gain_ref):
    blocks = []
    for step, pair_ref in steps:
        columns = pair_columns(step, 2 * pair_ref.shape[2])
        blocks.append((split_pair(pair_ref, gain_ref, columns), columns))
    return blocks


def normed_blocks(steps, gain_ref, inv_root):
    blocks = []
    for step, pair_ref in steps:
        columns = pair_columns(step, 2 * pair_ref.shape[2])
        blocks.append((normed_pair(pair_ref, gain_ref, columns, inv_root), columns))
    return blocks


def early_project_kernel(step, pair_ref, gain_ref, *refs):
    weight_refs, before_refs, total_ref = refs[:4], refs[4:-1], refs[-1]

    def finish(place, total):
        total = joined(total)
        for ref in before_refs:
            total = total + ref[:, place]
        total_ref[:, place] = total

    project_blocks(split_blocks(((step(), pair_ref),), gain_ref), weight_refs, finish)


def inverse_root(pair_refs):
    squares, width = 0.0, 0
    for pair_ref in pair_refs:
        rows = flat_pair(pair_ref)
        squares = squares + jnp.sum(rows * rows, axis=1, keepdims=True)
        width += rows.shape[1]
    return lax.rsqrt(squares / width + epsilon)


def project_kernel(chips, *refs):
    pair_refs, (early_ref, gain_ref) = refs[:chips], refs[chips : chips + 2]
    weight_refs = refs[chips + 2 : chips + 6]
    near_ref, mid_ref, far_ref, swap_ref, total_ref, made_ref = refs[chips + 6 :]
    core = lax.axis_index("tp")
    inv_root = inverse_root(pair_refs)

    def finish(place, total):
        total_ref[:, place] = early_ref[:, place] * inv_root + total

    project_blocks(normed_blocks(late_steps(pair_refs), gain_ref, inv_root), weight_refs, finish)
    heads, chan, _ = weight_refs[0].shape
    rows, lanes = total_ref.shape[0], 4 * chan
    product = total_ref[...]
    for head in range(heads):
        made_ref[pl.ds(head, rows, stride=heads), :] = product[:, head * lanes : (head + 1) * lanes]
    chip = lax.axis_index("kv")
    pairs = rows * heads // chips
    for step, sent_ref in placed_blocks(core, near_ref, mid_ref, far_ref, swap_ref):
        first = pl.multiple_of(lax.bitwise_xor(chip, step) * pairs, pairs)
        sent_ref[...] = made_ref[pl.ds(first, pairs), :].astype(jnp.bfloat16)


def sigmoid(x):
    small = jnp.exp(-jnp.abs(x))
    return jnp.where(x >= 0.0, 1.0, small) / (1.0 + small)


def readout_kernel(chips, *refs):
    got_refs, (bound_ref, state_ref, gain_ref) = refs[:chips], refs[chips : chips + 3]
    mixed_ref, key_ref, value_ref, placed_ref = refs[chips + 3 :]
    own_rows, heads, keys, _ = state_ref.shape
    chan = keys // chips
    chip, core = lax.axis_index("kv"), lax.axis_index("tp")
    for step, got_ref in placed_blocks(core, *got_refs):
        block = got_ref[...] if len(got_ref.shape) == 2 else got_ref[core]
        placed_ref[lax.bitwise_xor(chip, step)] = block.astype(jnp.float32)

    def channels(kind):
        return jnp.concatenate(
            [placed_ref[i][:, kind * chan : (kind + 1) * chan] for i in range(chips)], axis=1
        )

    pre_query, pre_forget, value_rows, pre_gate = (channels(kind) for kind in range(4))
    bound = jnp.concatenate([bound_ref[...]] * own_rows, axis=0)
    gain = jnp.concatenate([gain_ref[...]] * own_rows, axis=0)
    forget = bound + (1.0 - bound) * sigmoid(pre_forget)
    key_rows = (1.0 - bound) * sigmoid(-pre_forget)
    query = pre_query * sigmoid(pre_query)
    new_part = jnp.sum(query * key_rows, axis=1, keepdims=True) * value_rows
    weight = jnp.transpose(query * forget)
    old_parts = []
    for row in range(own_rows):
        for head in range(heads):
            pair = row * heads + head
            old_parts.append(
                jnp.sum(weight[:, pair : pair + 1] * state_ref[row, head], axis=0, keepdims=True)
            )
    readout = jnp.concatenate(old_parts, axis=0) + new_part
    inv_head = lax.rsqrt(jnp.mean(readout * readout, axis=1, keepdims=True) + epsilon)
    mixed = readout * inv_head * gain * (pre_gate * sigmoid(pre_gate))
    mixed_ref[...] = mixed.astype(jnp.bfloat16)
    key_ref[...] = key_rows
    value_ref[...] = value_rows


def state_kernel(key_ref, value_ref, state_ref, next_ref):
    own_rows, heads, _, _ = state_ref.shape
    key_cols = jnp.transpose(key_ref[...])
    for row in range(own_rows):
        for head in range(heads):
            pair = row * heads + head
            old = state_ref[row, head]
            next_ref[row, head] = old + key_cols[:, pair : pair + 1] * (
                value_ref[pair : pair + 1, :] - old
            )


def copy_out_kernel(made_ref, next_ref, done_ref):
    copy = pltpu.make_async_copy(made_ref, next_ref, done_ref)
    copy.start()
    copy.wait()


def stage_kernel(block_ref, staged_ref):
    staged_ref[...] = block_ref[...]


def out_kernel(chips, heads, *refs):
    pair_refs, (tokens_ref, weight_ref, residual_ref, placed_ref) = refs[:chips], refs[chips:]
    cores, pairs, values = pair_refs[0].shape
    own_rows = pairs // heads
    chip = lax.axis_index("kv")
    for step, pair_ref in placed_blocks(lax.axis_index("tp"), *pair_refs):
        first = pl.multiple_of(lax.bitwise_xor(chip, step) * (cores * pairs), cores * pairs)
        placed_ref[pl.ds(first, cores * pairs), :] = (
            pair_ref[...].astype(jnp.float32).reshape(-1, values)
        )
    blocks = []
    for core in range(cores):
        for head in range(heads):
            blocks.append(
                jnp.concatenate(
                    [
                        placed_ref[
                            pl.ds(core * pairs + row * heads + head, chips, stride=cores * pairs), :
                        ]
                        for row in range(own_rows)
                    ],
                    axis=0,
                )
            )
    mixed = jnp.concatenate(blocks, axis=1).astype(jnp.bfloat16)
    weight = weight_ref[...].reshape(-1, weight_ref.shape[2])
    projected = jnp.dot(mixed, weight, preferred_element_type=jnp.float32)
    ordered = [
        projected[row * chips + i : row * chips + i + 1]
        for i in range(chips)
        for row in range(own_rows)
    ]
    projected = jnp.concatenate(ordered, axis=0)
    residual_ref[...] = (tokens_ref[...].astype(jnp.float32) + projected).astype(jnp.bfloat16)


def down_part(hidden, down_ref, core, partial_ref):
    width = partial_ref.shape[2]
    chip = lax.axis_index("kv")
    far = lax.bitwise_xor(chip, far_step(core))
    columns = (2 * far, 2 * far + 1, 2 * lax.bitwise_xor(chip, 3) + core, 2 * chip + core)
    for slot, column in enumerate(columns[: partial_ref.shape[0]]):
        partial_ref[slot] = jnp.dot(
            hidden,
            down_ref[:, pl.ds(pl.multiple_of(column * width, width), width)],
            preferred_element_type=jnp.float32,
        )


def up_blocks(blocks, up_ref):
    total = None
    for rows, columns in blocks:
        part = jnp.dot(rows, up_ref[columns, :], preferred_element_type=jnp.float32)
        total = part if total is None else total + part
    return total


def early_up_kernel(step, pair_ref, gain_ref, up_ref, down_ref, *refs):
    del down_ref
    total = joined(up_blocks(split_blocks(((step(), pair_ref),), gain_ref), up_ref))
    for ref in refs[:-1]:
        total = total + ref[...]
    refs[-1][...] = total


def mixer_kernel(chips, *refs):
    pair_refs, (early_ref, gain_ref, up_ref, down_ref) = refs[:chips], refs[chips : chips + 4]
    hidden_ref, partial_ref = refs[chips + 4 :]
    inv_root = inverse_root(pair_refs)
    late = up_blocks(normed_blocks(late_steps(pair_refs), gain_ref, inv_root), up_ref)
    hidden = early_ref[...] * inv_root + late
    hidden = jnp.square(jnp.maximum(hidden, 0.0)).astype(jnp.bfloat16)
    hidden_ref[...] = hidden
    down_part(hidden, down_ref, 1 - lax.axis_index("tp"), partial_ref)


def own_part_kernel(hidden_ref, down_ref, partial_ref):
    down_part(hidden_ref[...], down_ref, lax.axis_index("tp"), partial_ref)


def mate_kept_kernel(hidden_ref, down_ref, kept_ref):
    width = kept_ref.shape[1]
    column = 2 * lax.axis_index("kv") + 1 - lax.axis_index("tp")
    kept_ref[...] = jnp.dot(
        hidden_ref[...],
        down_ref[:, pl.ds(pl.multiple_of(column * width, width), width)],
        preferred_element_type=jnp.float32,
    )


def chip_sum_kernel(own_ref, mate_ref, far_ref, mid_ref, kept_ref):
    for core in range(2):
        far_ref[core] = (own_ref[core] + mate_ref[core]).astype(jnp.bfloat16)
    mid_ref[...] = (own_ref[2] + mate_ref[2]).astype(jnp.bfloat16)
    kept_ref[...] = own_ref[3]


def last_kernel(residual_ref, kept_ref, mid_ref, far_ref, swapped_ref, mate_ref, output_ref):
    core = lax.axis_index("tp")
    total = kept_ref[...] + mate_ref[...]
    for block in (mid_ref[...], far_ref[core], swapped_ref[core]):
        total = total + block.astype(jnp.float32)
    output_ref[...] = (residual_ref[...].astype(jnp.float32) + total).astype(jnp.bfloat16)


MIB = 1 << 20
COST = (10**11, 10**11, 10**9, 10**9, 10**6, 10**6, 10**9, 10**6, 10**6, 10**9, 10**6)


def tiled_local(
    kv,
    tp,
    tokens,
    mix_gain,
    query_weight,
    forget_weight,
    value_weight,
    gate_weight,
    lower_bound,
    recurrent_state,
    head_gain,
    out_weight,
    mlp_gain,
    up_weight,
    down_weight,
):
    rows, width = tokens.shape
    heads, chan, _ = query_weight.shape
    own_rows, _, keys, values = recurrent_state.shape
    pairs = own_rows * heads
    shape = jax.ShapeDtypeStruct
    f32, bf16 = jnp.float32, jnp.bfloat16

    def permute(block, steps, swapped=False):
        hops = [
            (k * tp + t, (k ^ steps[t]) * tp + (1 - t if swapped else t))
            for k in range(kv)
            for t in range(tp)
        ]
        return lax.ppermute(block, group, hops)

    def other_core(block):
        return permute(block, (0, 0), True)

    def paired(block, mate, cost):
        return call(pair_kernel, shape((tp,) + block.shape, block.dtype), (block, mate), cost, MIB)

    def crossed(far, mid):
        got_far = permute(far, (1, 2))
        got_mid = permute(mid, (3, 3))
        return got_mid, got_far, permute(got_far, (0, 0), True)

    def gather_pairs(block, staged, cost):
        pair = paired(staged, other_core(block), cost)
        return (pair,) + crossed(pair, pair)

    def early_parts(kernel, got, operands, columns, cost):
        total = ()
        for place, step in ((0, near_step), (2, other_step), (3, swapped_step)):
            part = call(
                functools.partial(kernel, step),
                shape((rows, columns), f32),
                (got[place], *operands, *total),
                cost,
                14 * MIB,
            )
            total = (part,)
        return total[0]

    staged = call(stage_kernel, shape(tokens.shape, bf16), (tokens,), COST[4], MIB)
    pairs_of_rows = gather_pairs(tokens, staged, COST[0])
    mix_row = mix_gain.reshape(1, -1)
    projections = (query_weight, forget_weight, value_weight, gate_weight)
    early = early_parts(
        early_project_kernel, pairs_of_rows, (mix_row, *projections), 4 * heads * chan, COST[9]
    )
    near, mid, far, swap = call(
        functools.partial(project_kernel, kv),
        [shape((pairs, 4 * chan), bf16)] * kv,
        (*pairs_of_rows, early, mix_row, *projections),
        COST[1],
        14 * MIB,
        [pltpu.VMEM((rows, 4 * heads * chan), f32), pltpu.VMEM((rows * heads, 4 * chan), f32)],
    )
    got = (near,) + crossed(paired(far, other_core(swap), COST[4]), mid)
    mixed, key_rows, value_rows = call(
        functools.partial(readout_kernel, kv),
        [shape((pairs, values), bf16), shape((pairs, keys), f32), shape((pairs, values), f32)],
        (*got, lower_bound, recurrent_state, head_gain),
        COST[2],
        14 * MIB,
        [pltpu.VMEM((kv, pairs, 4 * chan), f32)],
    )
    next_state = call(
        state_kernel,
        pltpu.VMEM(recurrent_state.shape, f32),
        (key_rows, value_rows, recurrent_state),
        COST[3],
        4 * MIB,
    )
    next_state = pl.pallas_call(
        copy_out_kernel,
        out_shape=shape(recurrent_state.shape, f32),
        in_specs=[whole],
        out_specs=pl.BlockSpec(memory_space=pl.ANY),
        scratch_shapes=[pltpu.SemaphoreType.DMA],
        compiler_params=pltpu.CompilerParams(vmem_limit_bytes=MIB),
        cost_estimate=pl.CostEstimate(flops=COST[3], bytes_accessed=0, transcendentals=0),
    )(next_state)
    residual = call(
        functools.partial(out_kernel, kv, heads),
        shape((rows, width), bf16),
        (*gather_pairs(mixed, mixed, COST[4]), tokens, out_weight),
        COST[4],
        14 * MIB,
        [pltpu.VMEM((kv * tp * pairs, values), f32)],
    )
    pairs_of_rows = gather_pairs(residual, residual, COST[4])
    mlp_row = mlp_gain.reshape(1, -1)
    early = early_parts(
        early_up_kernel, pairs_of_rows, (mlp_row, up_weight, down_weight), up_weight.shape[1], COST[10]
    )
    hidden, mate_part = call(
        functools.partial(mixer_kernel, kv),
        [shape((rows, up_weight.shape[1]), bf16), shape((kv - 1, rows, width), f32)],
        (*pairs_of_rows, early, mlp_row, up_weight, down_weight),
        COST[5],
        14 * MIB,
    )
    own_part = call(
        own_part_kernel, shape((kv, rows, width), f32), (hidden, down_weight), COST[6], 14 * MIB
    )
    far, mid, kept = call(
        chip_sum_kernel,
        [shape((tp, rows, width), bf16), shape((rows, width), bf16), shape((rows, width), f32)],
        (own_part, other_core(mate_part)),
        COST[7],
        MIB,
    )
    sums = crossed(far, mid)
    mate_kept = call(
        mate_kept_kernel, shape((rows, width), f32), (hidden, down_weight), COST[7], 14 * MIB
    )
    mate_kept = other_core(mate_kept)
    layer_output = call(
        last_kernel, shape((rows, width), bf16), (residual, kept, *sums, mate_kept), COST[8], MIB
    )
    return (layer_output, next_state)


def tiles(kv, tp, tokens, query_weight):
    rows, width = tokens.shape
    aligned = rows % 8 == 0 and width % 128 == 0 and query_weight.shape[1] % 32 == 0
    return aligned and tp == 2 and kv == 4


def solution(mesh):
    placed = (
        P("dp", ("kv", "tp")),
        P(),
        P("tp", "kv", None),
        P("tp", "kv", None),
        P("tp", "kv", None),
        P("tp", "kv", None),
        P("tp", None),
        P(("dp", "kv"), "tp", None, None),
        P("tp", None),
        P(None, None, ("kv", "tp")),
        P(),
        P(None, ("kv", "tp")),
        P(("kv", "tp"), None),
    )

    def body(*arrays):
        kv, tp = mesh.shape["kv"], mesh.shape["tp"]
        run = tiled_local if tiles(kv, tp, arrays[0], arrays[2]) else local
        return run(kv, tp, *arrays)

    return jax.shard_map(
        body,
        mesh=mesh,
        in_specs=placed,
        out_specs=(P("dp", ("kv", "tp")), P(("dp", "kv"), "tp", None, None)),
        check_vma=False,
    )
```
